32 devices in a mesh: ep: 16 (over z, y, core), tp: 2 (over x).
Axes of the slice: x: 2, y: 2, z: 4, core: 2. Of those that a mesh axis runs over, the one named last changes fastest.
Arguments:
- tokens: bfloat16 [128, 1024], P('ep'), may hold values from -6 to 6
- ssm_state: float32 [128, 32, 64, 128], P('ep', 'tp'), may hold values from -6 to 6
- conv_x: bfloat16 [128, 3, 2048], P('ep', None, 'tp'), may hold values from -6 to 6
- conv_b: bfloat16 [128, 3, 1024], P('ep', None, 'tp'), may hold values from -6 to 6
- conv_c: bfloat16 [128, 3, 1024], P('ep', None, 'tp'), may hold values from -6 to 6
- w_x: bfloat16 [1024, 2048], P(None, 'tp'), may hold values from -0.1875 to 0.1875
- w_z: bfloat16 [1024, 2048], P(None, 'tp'), may hold values from -0.1875 to 0.1875
- w_b: bfloat16 [1024, 1024], P(None, 'tp'), may hold values from -0.1875 to 0.1875
- w_c: bfloat16 [1024, 1024], P(None, 'tp'), may hold values from -0.1875 to 0.1875
- w_dt: bfloat16 [1024, 32], replicated, may hold values from -0.1875 to 0.1875
- dt_bias: float32 [32], P('tp'), may hold values from -2 to 1
- a_log: float32 [32], P('tp'), may hold values from -3 to 1
- d_skip: float32 [32], P('tp'), may hold values from 0.1 to 1.9
- taps_x: bfloat16 [4, 2048], P(None, 'tp'), may hold values from -3 to 3
- taps_b: bfloat16 [4, 1024], P(None, 'tp'), may hold values from -3 to 3
- taps_c: bfloat16 [4, 1024], P(None, 'tp'), may hold values from -3 to 3
- norm1_gain: float32 [1024], replicated, may hold values from 0.1 to 1.9
- group_gain: float32 [2048], P('tp'), may hold values from 0.1 to 1.9
- w_out: bfloat16 [2048, 1024], P('tp'), may hold values from -0.125 to 0.125
- norm2_gain: float32 [1024], replicated, may hold values from 0.1 to 1.9
- route_ids: int32 [128, 6], P('ep'), may hold values from 0 to 15, all different within a row; in each aligned block of 8 rows (0 to 7, 8 to 15, ...) at most 6 rows name the same one
- route_weights: float32 [128, 6], P('ep'), may hold values from 0.1 to 1
- exp_gate: bfloat16 [16, 1024, 512], P('ep', None, 'tp'), may hold values from -0.1875 to 0.1875
- exp_up: bfloat16 [16, 1024, 512], P('ep', None, 'tp'), may hold values from -0.1875 to 0.1875
- exp_down: bfloat16 [16, 512, 1024], P('ep', 'tp'), may hold values from -0.25 to 0.25
- dense_gate: bfloat16 [1024, 1024], P('ep', 'tp'), may hold values from -0.1875 to 0.1875
- dense_up: bfloat16 [1024, 1024], P('ep', 'tp'), may hold values from -0.1875 to 0.1875
- dense_down: bfloat16 [1024, 1024], P('tp', 'ep'), may hold values from -0.1875 to 0.1875
- branch_gate: bfloat16 [1024], replicated, may hold values from -0.375 to 0.375
Outputs:
- mixed: bfloat16 [128, 1024], P('ep', 'tp')
- state_next: float32 [128, 32, 64, 128], P('ep', 'tp')
- conv_x_next: bfloat16 [128, 3, 2048], P('ep', None, 'tp')
- conv_b_next: bfloat16 [128, 3, 1024], P('ep', None, 'tp')
- conv_c_next: bfloat16 [128, 3, 1024], P('ep', None, 'tp')
The draws below stay inside these ranges and needn't reach their ends.
Inputs may be any that keep to these rules, and one draw needn't show every extreme that they name: `route_ids`: each row names 6 different experts. Among the rows of one device no expert is named by more than 6 rows, a bound that some block reaches.
All inputs are finite; a program needn't handle non-finite values.
Results may differ from the reference program's by a relative error of at most 0.019.
Values may be sent and summed in bfloat16 or wider, within the bound.
No kernel may reach another device: no remote copies, remote signals or barrier semaphores. Data moves between devices by JAX's collectives and lax.ppermute only.
A program may use at most 64 MiB of HBM per device.

```python
import math
import jax
import jax.numpy as jnp
import numpy as np
from jax import lax

D = 1024
HEADS = 32
HEAD_DIM = 64
STATE_DIM = 128
CONV_TAPS = 4
EXPERT_FF = 512
DENSE_FF = 1024
TOP_K = 6
SEQ_DEV = 8
INNER = 2048
STATE_COLS = 1024
TOKENS = 128
EXPERTS = 16
CAP = 6
N_EP = 16
N_TP = 2


def steps_of(own_key, dims, pieces, least, top_value):
    level, own = 1.0, jax.random.fold_in(own_key, 6)
    for position, parts in pieces:
        draws = jnp.exp(jax.random.uniform(jax.random.fold_in(own, position), (parts,), jnp.float32, least / len(pieces), top_value / len(pieces)))
        level = level * jnp.repeat(draws, dims[position] // parts).reshape([-1 if axis == position else 1 for axis in range(len(dims))])
    return level


def shared_out(stream_key, own, number, rows, amount, top, most, slope):
    order = jax.random.permutation(stream_key, amount)
    heavy_load, ordinary = shares(amount, rows * top, most, slope, True), shares(amount, rows * top, most, slope, False)
    places = jnp.arange(amount)

    def named(sizes, turn):
        used = int((sizes > 0).sum())
        fixed = max(1, used // 4)
        passed = fixed + (places - fixed + turn * (used - fixed)) % max(1, amount - fixed)
        return jnp.zeros((amount,), jnp.int32).at[order[jnp.where(places < fixed, places, passed)]].set(jnp.asarray(sizes, jnp.int32))

    sizes = jnp.where(number % 4 == 0, named(heavy_load, number // 4), named(ordinary, number - number // 4 - 1))
    mixed = jax.random.permutation(jax.random.fold_in(own, 3), amount)
    source_of, receiver = mixed[0:amount // 2 * 2:2], mixed[1:amount // 2 * 2:2]
    margin = jnp.minimum(sizes[source_of] - 1, most - sizes[receiver]) // 2
    margin = jnp.where((source_of == order[0]) | (receiver == order[0]) | (sizes[receiver] == 0), 0, jnp.maximum(margin, 0))
    passed = jax.random.randint(jax.random.fold_in(own, 4), (amount // 2,), 0, 1 << 20) % (margin + 1)
    sizes = sizes.at[source_of].add(-passed).at[receiver].add(passed)
    items = jnp.searchsorted(jnp.cumsum(sizes), jnp.arange(rows * top), side="right").astype(jnp.int32)
    table = items.reshape(top, rows).T
    table = table[jax.random.permutation(jax.random.fold_in(own, 1), rows)]
    turn = jax.random.randint(jax.random.fold_in(own, 2), (rows, 1), 0, top)
    return jnp.take_along_axis(table, (jnp.arange(top)[None, :] + turn) % top, axis=1)


def shares(count, total, bound, slope, full):
    loads = [(1 << 20) // math.isqrt(standing ** slope) + 1 for standing in range(1, count + 1)]
    largest = bound if full else min(bound, max(-(-total // count), total * loads[0] // sum(loads)))
    least = 1 if total - largest >= count - 1 else 0
    holding, surplus = [largest] + [least] * (count - 1), total - largest - least * (count - 1)
    while surplus > 0:
        candidates = [i for i in range(1, count) if holding[i] < largest] or [i for i in range(1, count) if holding[i] < bound]
        mass, left = sum([loads[i] for i in candidates]), surplus
        for i in candidates:
            extra = min(bound - holding[i], max(1, left * loads[i] // mass), surplus)
            holding[i] = holding[i] + extra
            surplus = surplus - extra
    return np.array(holding)


def scatter_about(own_key, shape, scale, most, pieces=(), kind=jnp.bfloat16):
    drawn = jax.random.normal(own_key, shape, jnp.float32) * scale
    if len(pieces) > 0:
        drawn = steps_of(own_key, shape, pieces, -0.22, 0.18) * drawn
    return jnp.clip(drawn, min=-most, max=most).astype(kind)


def setup_inputs(seed: int = 0) -> dict:
    keys = jax.random.split(jax.random.key(seed), 30)
    tokens = scatter_about(keys[0], (TOKENS, D), 1.0, 6.0, ((0, 16),))
    ssm_state = scatter_about(keys[1], (TOKENS, HEADS, HEAD_DIM, STATE_DIM), 1.0, 6.0, ((0, 16), (1, 2)), jnp.float32)
    conv_x = scatter_about(keys[2], (TOKENS, CONV_TAPS - 1, INNER), 1.0, 6.0, ((0, 16), (2, 2)))
    conv_b = scatter_about(keys[3], (TOKENS, CONV_TAPS - 1, STATE_COLS), 1.0, 6.0, ((0, 16), (2, 2)))
    conv_c = scatter_about(keys[4], (TOKENS, CONV_TAPS - 1, STATE_COLS), 1.0, 6.0, ((0, 16), (2, 2)))
    w_x = scatter_about(keys[5], (D, INNER), D ** -0.5, 0.1875, ((1, 2),))
    w_z = scatter_about(keys[6], (D, INNER), D ** -0.5, 0.1875, ((1, 2),))
    w_b = scatter_about(keys[7], (D, STATE_COLS), D ** -0.5, 0.1875, ((1, 2),))
    w_c = scatter_about(keys[8], (D, STATE_COLS), D ** -0.5, 0.1875, ((1, 2),))
    w_dt = scatter_about(keys[9], (D, HEADS), D ** -0.5, 0.1875)
    dt_bias = jnp.clip(-2.0 + 3.0 * jax.random.uniform(keys[10], (HEADS,), jnp.float32) ** steps_of(keys[10], (HEADS,), ((0, 2),), -0.2, 0.2), -2.0, 1.0)
    a_log = jnp.clip(-3.0 + 4.0 * jax.random.uniform(keys[11], (HEADS,), jnp.float32) ** steps_of(keys[11], (HEADS,), ((0, 2),), -0.2, 0.2), -3.0, 1.0)
    d_skip = jnp.clip(1.0 + 0.18 * jax.random.normal(keys[12], (HEADS,), jnp.float32), 0.1, 1.9)
    taps_x = scatter_about(keys[13], (CONV_TAPS, INNER), CONV_TAPS ** -0.5, 3.0, ((1, 2),))
    taps_b = scatter_about(keys[14], (CONV_TAPS, STATE_COLS), CONV_TAPS ** -0.5, 3.0, ((1, 2),))
    taps_c = scatter_about(keys[15], (CONV_TAPS, STATE_COLS), CONV_TAPS ** -0.5, 3.0, ((1, 2),))
    norm1_gain = jnp.clip(1.0 + 0.18 * jax.random.normal(keys[16], (D,), jnp.float32), 0.1, 1.9)
    group_gain = jnp.clip(1.0 + 0.18 * jax.random.normal(keys[17], (INNER,), jnp.float32), 0.1, 1.9)
    w_out = scatter_about(keys[18], (INNER, D), INNER ** -0.5, 0.125, ((0, 2),))
    norm2_gain = jnp.clip(1.0 + 0.18 * jax.random.normal(keys[19], (D,), jnp.float32), 0.1, 1.9)
    route_ids_keys = jax.random.split(jax.random.fold_in(keys[20], 1), TOKENS // SEQ_DEV)
    route_ids_turns = jax.random.permutation(jax.random.fold_in(keys[20], 3), TOKENS // SEQ_DEV)
    route_ids = jax.vmap(lambda own, number: shared_out(jax.random.fold_in(keys[20], 2), own, number, SEQ_DEV, EXPERTS, TOP_K, CAP, 2))(route_ids_keys, route_ids_turns).reshape((TOKENS, TOP_K))
    route_weights = jnp.clip(0.1 + 0.9 * jax.random.uniform(keys[21], (TOKENS, TOP_K), jnp.float32) ** steps_of(keys[21], (TOKENS, TOP_K), ((0, 16),), -0.2, 0.2), 0.1, 1.0)
    exp_gate = scatter_about(keys[22], (EXPERTS, D, EXPERT_FF), D ** -0.5, 0.1875, ((0, 16), (2, 2)))
    exp_up = scatter_about(keys[23], (EXPERTS, D, EXPERT_FF), D ** -0.5, 0.1875, ((0, 16), (2, 2)))
    exp_down = scatter_about(keys[24], (EXPERTS, EXPERT_FF, D), EXPERT_FF ** -0.5, 0.25, ((0, 16), (1, 2)))
    dense_gate = scatter_about(keys[25], (D, DENSE_FF), D ** -0.5, 0.1875, ((0, 16), (1, 2)))
    dense_up = scatter_about(keys[26], (D, DENSE_FF), D ** -0.5, 0.1875, ((0, 16), (1, 2)))
    dense_down = scatter_about(keys[27], (DENSE_FF, D), DENSE_FF ** -0.5, 0.1875, ((0, 2), (1, 16)))
    branch_gate = scatter_about(keys[28], (D,), (D // 4) ** -0.5, 0.375)
    return dict(tokens=tokens, ssm_state=ssm_state, conv_x=conv_x, conv_b=conv_b, conv_c=conv_c, w_x=w_x, w_z=w_z, w_b=w_b, w_c=w_c, w_dt=w_dt, dt_bias=dt_bias, a_log=a_log, d_skip=d_skip, taps_x=taps_x, taps_b=taps_b, taps_c=taps_c, norm1_gain=norm1_gain, group_gain=group_gain, w_out=w_out, norm2_gain=norm2_gain, route_ids=route_ids, route_weights=route_weights, exp_gate=exp_gate, exp_up=exp_up, exp_down=exp_down, dense_gate=dense_gate, dense_up=dense_up, dense_down=dense_down, branch_gate=branch_gate)


epsilon = 1e-06

def rms_rows(values, gain):
    return values * lax.rsqrt(lax.optimization_barrier(jnp.mean(values * values, axis=-1, keepdims=True)) + epsilon) * gain

def blocked_sum(left, right, blocks):
    width = left.shape[1] // blocks
    total = jnp.zeros((left.shape[0], right.shape[1]), jnp.float32)
    for index in range(blocks):
        partial_term = jnp.dot(left[:, index * width:(index + 1) * width], right[index * width:(index + 1) * width], preferred_element_type=jnp.float32)
        rounded = lax.optimization_barrier(partial_term.astype(jnp.bfloat16))
        total = total + rounded.astype(jnp.float32)
    return total

def short_conv(previous, fresh, taps):
    window = jnp.concatenate((previous, fresh[:, None]), axis=1)
    summed = lax.optimization_barrier(jnp.sum(window.astype(jnp.float32) * taps.astype(jnp.float32)[None], axis=1))
    return (jax.nn.silu(summed), window[:, 1:])

def mixer_core(x_new, z_new, b_new, c_new, dt_raw, ssm_state, conv_x, conv_b, conv_c, dt_bias, a_log, d_skip, taps_x, taps_b, taps_c, group_gain):
    seqs, heads, head_dim, state_dim = ssm_state.shape
    groups = b_new.shape[1] // state_dim
    x_conv, conv_x_next = short_conv(conv_x, x_new, taps_x)
    b_conv, conv_b_next = short_conv(conv_b, b_new, taps_b)
    c_conv, conv_c_next = short_conv(conv_c, c_new, taps_c)
    x_heads = x_conv.reshape(seqs, heads, head_dim)
    b_heads = jnp.repeat(b_conv.reshape(seqs, groups, state_dim), heads // groups, axis=1)
    c_heads = jnp.repeat(c_conv.reshape(seqs, groups, state_dim), heads // groups, axis=1)
    step = jax.nn.softplus(dt_raw + dt_bias)
    decay = jnp.exp(-step * jnp.exp(a_log))
    state_next = decay[:, :, None, None] * ssm_state + (step[:, :, None] * x_heads)[:, :, :, None] * b_heads[:, :, None, :]
    readout = jnp.einsum('shpn,shn->shp', state_next, c_heads, precision=lax.Precision.HIGHEST) + d_skip[None, :, None] * x_heads
    gated = readout.reshape(seqs, heads * head_dim) * jax.nn.silu(z_new.astype(jnp.float32))
    grouped = gated.reshape(seqs, groups, -1)
    grouped = grouped * lax.rsqrt(lax.optimization_barrier(jnp.mean(grouped * grouped, axis=-1, keepdims=True)) + epsilon)
    mixed_heads = (grouped.reshape(seqs, heads * head_dim) * group_gain).astype(jnp.bfloat16)
    return (mixed_heads, state_next, conv_x_next, conv_b_next, conv_c_next)

def reference(tokens, ssm_state, conv_x, conv_b, conv_c, w_x, w_z, w_b, w_c, w_dt, dt_bias, a_log, d_skip, taps_x, taps_b, taps_c, norm1_gain, group_gain, w_out, norm2_gain, route_ids, route_weights, exp_gate, exp_up, exp_down, dense_gate, dense_up, dense_down, branch_gate):
    stream = tokens.astype(jnp.float32)
    normed = rms_rows(stream, norm1_gain).astype(jnp.bfloat16)
    x_new = jnp.dot(normed, w_x, preferred_element_type=jnp.float32).astype(jnp.bfloat16)
    z_new = jnp.dot(normed, w_z, preferred_element_type=jnp.float32).astype(jnp.bfloat16)
    b_new = jnp.dot(normed, w_b, preferred_element_type=jnp.float32).astype(jnp.bfloat16)
    c_new = jnp.dot(normed, w_c, preferred_element_type=jnp.float32).astype(jnp.bfloat16)
    dt_raw = jnp.dot(normed, w_dt, preferred_element_type=jnp.float32)
    mixed_heads, state_next, conv_x_next, conv_b_next, conv_c_next = mixer_core(x_new, z_new, b_new, c_new, dt_raw, ssm_state, conv_x, conv_b, conv_c, dt_bias, a_log, d_skip, taps_x, taps_b, taps_c, group_gain)
    residual = (stream + blocked_sum(mixed_heads, w_out, N_TP)).astype(jnp.bfloat16)
    normed2 = rms_rows(residual.astype(jnp.float32), norm2_gain).astype(jnp.bfloat16)
    expert_iota = jnp.arange(EXPERTS, dtype=jnp.int32)
    matches = route_ids[:, :, None] == expert_iota[None, None, :]
    routed = lax.optimization_barrier(jnp.sum(matches.astype(jnp.int32), axis=1))
    weight_of = lax.optimization_barrier(jnp.sum(jnp.where(matches, route_weights[:, :, None], jnp.float32(0.0)), axis=1))
    blocked = routed.reshape(N_EP, SEQ_DEV, EXPERTS)
    ranked = (jnp.cumsum(blocked, axis=1) - blocked).reshape(TOKENS, EXPERTS)
    token_iota = jnp.arange(TOKENS, dtype=jnp.int32)
    source = token_iota // SEQ_DEV
    total_slots = EXPERTS * N_EP * CAP
    target = expert_iota[None, :] * (N_EP * CAP) + source[:, None] * CAP + ranked
    target = jnp.where(routed > 0, target, total_slots).astype(jnp.int32)
    owners = jnp.broadcast_to(token_iota[:, None], (TOKENS, EXPERTS)).reshape(-1)
    slot_token = jnp.zeros((total_slots,), jnp.int32).at[target.reshape(-1)].set(owners, mode='drop')
    slot_weight = jnp.zeros((total_slots,), jnp.float32).at[target.reshape(-1)].set(weight_of.reshape(-1), mode='drop')

    def run_expert(operands):
        index_rows, gate_weight, up_weight, down_weight = operands
        chosen = normed2[index_rows]
        gate_pre = jnp.dot(chosen, gate_weight, preferred_element_type=jnp.float32)
        up_pre = jnp.dot(chosen, up_weight, preferred_element_type=jnp.float32)
        active = (jax.nn.silu(gate_pre) * up_pre).astype(jnp.bfloat16)
        return blocked_sum(active, down_weight, N_TP).astype(jnp.bfloat16)
    slot_out = lax.map(run_expert, (slot_token.reshape(EXPERTS, N_EP * CAP), exp_gate, exp_up, exp_down))
    expert_sum = jnp.zeros((TOKENS, D), jnp.float32).at[slot_token].add(slot_weight[:, None] * slot_out.reshape(total_slots, D).astype(jnp.float32))
    dense_pre = jnp.dot(normed2, dense_gate, preferred_element_type=jnp.float32)
    dense_lift = jnp.dot(normed2, dense_up, preferred_element_type=jnp.float32)
    dense_active = (jax.nn.silu(dense_pre) * dense_lift).astype(jnp.bfloat16)
    dense_out = blocked_sum(dense_active, dense_down, N_TP)
    branch = jax.nn.sigmoid(jnp.dot(normed2, branch_gate[:, None], preferred_element_type=jnp.float32))
    mixed = (residual.astype(jnp.float32) + expert_sum + branch * dense_out).astype(jnp.bfloat16)
    return (mixed, state_next, conv_x_next, conv_b_next, conv_c_next)
```

```python
import functools
import math

import jax
import jax.numpy as jnp
from jax import lax
from jax.experimental import pallas as pl
from jax.experimental.pallas import tpu as pltpu
from jax.sharding import PartitionSpec as P

epsilon = 1e-06
f32 = jnp.float32
bf16 = jnp.bfloat16
VMEM = pl.BlockSpec(memory_space=pltpu.VMEM)
SMEM = pl.BlockSpec(memory_space=pltpu.SMEM)
HBM = pl.BlockSpec(memory_space=pltpu.HBM)
MIB = 1 << 20


def dot(left, right):
    return lax.dot_general(left, right, (((1,), (0,)), ((), ())), preferred_element_type=f32)


def dot_nt(left, right):
    return lax.dot_general(left, right, (((1,), (1,)), ((), ())), preferred_element_type=f32)


def silu(value):
    return value / (1.0 + jnp.exp(-value))


def sigmoid(value):
    return 1.0 / (1.0 + jnp.exp(-value))


def rms_rows(values, gain):
    return values * lax.rsqrt(jnp.mean(values * values, axis=-1, keepdims=True) + epsilon) * gain


def spread_heads(values, width):
    rows, heads = values.shape
    return jnp.concatenate(
        [jnp.broadcast_to(values[:, h : h + 1], (rows, width)) for h in range(heads)], axis=1
    )


def pack_kernel(gate_ref, up_ref, down_ref, ids_ref, weights_ref, out_ref, *, dests):
    rows, hidden = gate_ref.shape
    share = hidden // dests
    lanes = out_ref.shape[2]
    seqs, top_count = ids_ref.shape
    gate = gate_ref[...].astype(f32)
    up = up_ref[...].astype(f32)
    down = down_ref[...].astype(f32).T
    ids = ids_ref[...]
    weights = weights_ref[...]
    expert = lax.broadcasted_iota(jnp.int32, (seqs, dests), 1)
    weight_of = jnp.zeros((seqs, dests), f32)
    for k in range(top_count):
        weight_of += jnp.where(ids[:, k : k + 1] == expert, weights[:, k : k + 1], 0.0)
    high = weight_of.astype(bf16).astype(f32)
    low = weight_of - high
    if rows > seqs:
        rest = jnp.zeros((rows - seqs, dests), f32)
        high = jnp.concatenate((high, rest), axis=0)
        low = jnp.concatenate((low, rest), axis=0)
    for j in range(dests):
        part = slice(j * share, (j + 1) * share)
        block = [gate[:, part], up[:, part], down[:, part], high[:, j : j + 1], low[:, j : j + 1]]
        spare = lanes - 3 * share - 2
        if spare:
            block.append(jnp.zeros((rows, spare), f32))
        out_ref[j] = jnp.concatenate(block, axis=1).astype(bf16)


def mixer_kernel(
    tp_ref,
    tokens_ref,
    gain_ref,
    w_dt_ref,
    dt_bias_ref,
    a_log_ref,
    d_skip_ref,
    taps_x_ref,
    taps_b_ref,
    taps_c_ref,
    group_gain_ref,
    conv_x_ref,
    conv_b_ref,
    conv_c_ref,
    w_x_hbm,
    w_z_hbm,
    w_b_hbm,
    w_c_hbm,
    w_out_hbm,
    state_hbm,
    part_ref,
    conv_x_out,
    conv_b_out,
    conv_c_out,
    state_out,
    w_x,
    w_z,
    w_b,
    w_c,
    w_out,
    state,
    in_sems,
    state_sems,
    out_sems,
    *,
    n_tp,
):
    seqs, heads, head_dim, state_dim = state.shape
    channels = heads * head_dim
    groups = w_b.shape[1] // state_dim
    per_group = heads // groups
    width = channels // groups
    copy = pltpu.make_async_copy
    moves = {}
    for index, (name, source, target) in enumerate(
        (("x", w_x_hbm, w_x), ("b", w_b_hbm, w_b), ("c", w_c_hbm, w_c))
    ):
        moves[name] = copy(source, target, in_sems.at[index])
        moves[name].start()
    loads = [copy(state_hbm.at[s], state.at[s], state_sems.at[s]) for s in range(seqs)]
    stores = [copy(state.at[s], state_out.at[s], out_sems.at[s]) for s in range(seqs)]
    for load in loads:
        load.start()
    for index, (name, source, target) in enumerate((("z", w_z_hbm, w_z), ("o", w_out_hbm, w_out))):
        moves[name] = copy(source, target, in_sems.at[3 + index])
        moves[name].start()

    normed = rms_rows(tokens_ref[...].astype(f32), gain_ref[...]).astype(bf16)
    dt_all = dot(normed, w_dt_ref[...])
    own = tp_ref[0]
    dt_raw = jnp.zeros((seqs, heads), f32)
    for i in range(n_tp):
        dt_raw += jnp.where(own == i, dt_all[:, i * heads : (i + 1) * heads], 0.0)
    shifted = dt_raw + dt_bias_ref[...]
    step = jnp.maximum(shifted, 0.0) + jnp.log1p(jnp.exp(-jnp.abs(shifted)))
    decay = jnp.exp(-step * jnp.exp(a_log_ref[...]))

    def short_conv(previous_ref, fresh, taps_ref, out_ref):
        previous = previous_ref[...].astype(f32)
        taps = taps_ref[...].astype(f32)
        last = taps.shape[0] - 1
        total = jnp.sum(previous * taps[None, :last], axis=1) + fresh * taps[last:]
        out_ref[...] = jnp.concatenate((previous[:, 1:], fresh[:, None]), axis=1).astype(bf16)
        return silu(total)

    def projected(name, ref):
        moves[name].wait()
        return dot(normed, ref[...]).astype(bf16).astype(f32)

    xs = short_conv(conv_x_ref, projected("x", w_x), taps_x_ref, conv_x_out)
    bs = short_conv(conv_b_ref, projected("b", w_b), taps_b_ref, conv_b_out)
    cs = short_conv(conv_c_ref, projected("c", w_c), taps_c_ref, conv_c_out).astype(bf16)
    scaled = (spread_heads(step, head_dim) * xs).T
    row = lax.broadcasted_iota(jnp.int32, (seqs, width), 0)
    readout = [jnp.zeros((seqs, width), f32) for _ in range(groups)]
    for s in range(seqs):
        loads[s].wait()
        for g in range(groups):
            key = bs[s : s + 1, g * state_dim : (g + 1) * state_dim]
            fresh = []
            for h in range(g * per_group, (g + 1) * per_group):
                column = scaled[h * head_dim : (h + 1) * head_dim, s : s + 1]
                updated = decay[s : s + 1, h : h + 1] * state[s, h] + column * key
                state[s, h] = updated
                fresh.append(updated.astype(bf16))
            read = dot_nt(
                cs[:, g * state_dim : (g + 1) * state_dim], jnp.concatenate(fresh, axis=0)
            )
            readout[g] = jnp.where(row == s, read, readout[g])
        stores[s].start()
    z_gate = silu(projected("z", w_z))
    skip = spread_heads(d_skip_ref[...], head_dim) * xs
    mixed = []
    for g in range(groups):
        part = slice(g * width, (g + 1) * width)
        gated = (readout[g] + skip[:, part]) * z_gate[:, part]
        mixed.append(rms_rows(gated, group_gain_ref[:, part]).astype(bf16))
    moves["o"].wait()
    part_ref[...] = dot(jnp.concatenate(mixed, axis=1), w_out[...]).astype(bf16)
    for store in stores:
        store.wait()


def norm_kernel(tokens_ref, own_ref, other_ref, gain_ref, spread_ref, residual_ref):
    seqs = tokens_ref.shape[0]
    summed = own_ref[...].astype(f32) + other_ref[...].astype(f32)
    residual = (tokens_ref[...].astype(f32) + summed).astype(bf16)
    residual_ref[...] = residual
    normed = rms_rows(residual.astype(f32), gain_ref[...]).astype(bf16)
    for j in range(spread_ref.shape[0] // seqs):
        spread_ref[j * seqs : (j + 1) * seqs] = normed


def experts_kernel(
    rows_ref, packed_ref, gate_ref, up_ref, down_ref, branch_ref, out_ref, *, share, seqs, n_tp
):
    blocks, block_rows, lanes = packed_ref.shape
    count, model = rows_ref.shape
    rows = rows_ref[...]
    active = (silu(dot(rows, gate_ref[0])) * dot(rows, up_ref[0])).astype(bf16)
    routed = dot(active, down_ref[0])
    packed = packed_ref[...].reshape(blocks * block_rows, lanes)
    hidden = dot(rows, packed)
    lane = lax.broadcasted_iota(jnp.int32, (count, lanes), 1)
    dense = silu(pltpu.roll(hidden, 2 * share, 1)) * pltpu.roll(hidden, share, 1)
    chosen = (lane >= 2 * share) & (lane < 3 * share)
    dense = jnp.where(chosen, dense, 0.0).astype(bf16)
    dense_out = dot_nt(dense, packed)
    branch = sigmoid(
        jnp.sum(rows.astype(f32) * branch_ref[...].astype(f32), axis=1, keepdims=True)
    )
    table = jnp.concatenate(
        [packed_ref[i, :seqs].astype(f32) for i in range(blocks)], axis=0
    )
    weight = jnp.sum(
        jnp.where((lane >= 3 * share) & (lane < 3 * share + 2), table, 0.0), axis=1, keepdims=True
    )
    result = weight * routed + branch * dense_out
    half = model // n_tp
    for j in range(blocks):
        for q in range(n_tp):
            place = (j * n_tp + q) * seqs
            out_ref[place : place + seqs] = result[
                j * seqs : (j + 1) * seqs, q * half : (q + 1) * half
            ].astype(bf16)


def sum_kernel(tp_ref, parts_ref, residual_ref, out_ref, *, n_tp):
    seqs, half = out_ref.shape
    own = tp_ref[0]
    total = jnp.zeros((seqs, half), f32)
    for q in range(n_tp):
        total += jnp.where(
            own == q, residual_ref[:, q * half : (q + 1) * half].astype(f32), 0.0
        )
    for i in range(parts_ref.shape[0] // seqs):
        total += parts_ref[i * seqs : (i + 1) * seqs].astype(f32)
    out_ref[...] = total.astype(bf16)


def body(
    tokens,
    ssm_state,
    conv_x,
    conv_b,
    conv_c,
    w_x,
    w_z,
    w_b,
    w_c,
    w_dt,
    dt_bias,
    a_log,
    d_skip,
    taps_x,
    taps_b,
    taps_c,
    norm1_gain,
    group_gain,
    w_out,
    norm2_gain,
    route_ids,
    route_weights,
    exp_gate,
    exp_up,
    exp_down,
    dense_gate,
    dense_up,
    dense_down,
    branch_gate,
):
    seqs, model = tokens.shape
    n_ep = lax.axis_size("ep")
    n_tp = lax.axis_size("tp")
    tp_index = lax.axis_index("tp").astype(jnp.int32)[None]
    sds = jax.ShapeDtypeStruct

    rows, hidden = dense_gate.shape
    share = hidden // n_ep
    lanes = 128 * math.ceil((3 * share + 2) / 128)
    packed = pl.pallas_call(
        functools.partial(pack_kernel, dests=n_ep),
        out_shape=sds((n_ep, rows, lanes), bf16),
        in_specs=[VMEM] * 5,
        out_specs=VMEM,
        name="pack",
    )(dense_gate, dense_up, dense_down, route_ids, route_weights)
    packed = lax.all_to_all(packed, "ep", split_axis=0, concat_axis=0, tiled=True)

    part, conv_x_next, conv_b_next, conv_c_next, state_next = pl.pallas_call(
        functools.partial(mixer_kernel, n_tp=n_tp),
        out_shape=(
            sds((seqs, model), bf16),
            sds(conv_x.shape, bf16),
            sds(conv_b.shape, bf16),
            sds(conv_c.shape, bf16),
            sds(ssm_state.shape, f32),
        ),
        in_specs=[SMEM] + [VMEM] * 13 + [HBM] * 6,
        out_specs=(VMEM, VMEM, VMEM, VMEM, HBM),
        scratch_shapes=[
            pltpu.VMEM(w_x.shape, bf16),
            pltpu.VMEM(w_z.shape, bf16),
            pltpu.VMEM(w_b.shape, bf16),
            pltpu.VMEM(w_c.shape, bf16),
            pltpu.VMEM(w_out.shape, bf16),
            pltpu.VMEM(ssm_state.shape, f32),
            pltpu.SemaphoreType.DMA((5,)),
            pltpu.SemaphoreType.DMA((seqs,)),
            pltpu.SemaphoreType.DMA((seqs,)),
        ],
        compiler_params=pltpu.CompilerParams(vmem_limit_bytes=30 * MIB),
        name="mixer",
    )(
        tp_index,
        tokens,
        norm1_gain[None],
        w_dt,
        dt_bias[None],
        a_log[None],
        d_skip[None],
        taps_x,
        taps_b,
        taps_c,
        group_gain[None],
        conv_x,
        conv_b,
        conv_c,
        w_x,
        w_z,
        w_b,
        w_c,
        w_out,
        ssm_state,
    )

    if n_tp == 2:
        other = lax.ppermute(part, "tp", [(0, 1), (1, 0)])
    else:
        gathered = lax.all_gather(part, "tp", axis=0).astype(f32)
        total = gathered[0]
        for i in range(1, n_tp):
            total = total + gathered[i]
        other = total - part.astype(f32)

    spread, residual = pl.pallas_call(
        norm_kernel,
        out_shape=(sds((n_ep * seqs, model), bf16), sds((seqs, model), bf16)),
        in_specs=[VMEM] * 4,
        out_specs=(VMEM, VMEM),
        name="norm",
    )(tokens, part, other, norm2_gain[None])
    everyone = lax.all_to_all(spread, "ep", split_axis=0, concat_axis=0, tiled=True)

    outgoing = pl.pallas_call(
        functools.partial(experts_kernel, share=share, seqs=seqs, n_tp=n_tp),
        out_shape=sds((n_ep * n_tp * seqs, model // n_tp), bf16),
        in_specs=[VMEM] * 6,
        out_specs=VMEM,
        name="experts",
    )(everyone, packed, exp_gate, exp_up, exp_down, branch_gate[None])
    parts = lax.all_to_all(outgoing, ("ep", "tp"), split_axis=0, concat_axis=0, tiled=True)

    mixed = pl.pallas_call(
        functools.partial(sum_kernel, n_tp=n_tp),
        out_shape=sds((seqs, model // n_tp), bf16),
        in_specs=[SMEM, VMEM, VMEM],
        out_specs=VMEM,
        name="total",
    )(tp_index, parts, residual)
    return (mixed, state_next, conv_x_next, conv_b_next, conv_c_next)


def solution(mesh):
    return jax.shard_map(
        body,
        mesh=mesh,
        in_specs=(
            P("ep", None),
            P("ep", "tp", None, None),
            P("ep", None, "tp"),
            P("ep", None, "tp"),
            P("ep", None, "tp"),
            P(None, "tp"),
            P(None, "tp"),
            P(None, "tp"),
            P(None, "tp"),
            P(),
            P("tp"),
            P("tp"),
            P("tp"),
            P(None, "tp"),
            P(None, "tp"),
            P(None, "tp"),
            P(),
            P("tp"),
            P("tp", None),
            P(),
            P("ep", None),
            P("ep", None),
            P("ep", None, "tp"),
            P("ep", None, "tp"),
            P("ep", "tp", None),
            P("ep", "tp"),
            P("ep", "tp"),
            P("tp", "ep"),
            P(),
        ),
        out_specs=(
            P("ep", "tp"),
            P("ep", "tp", None, None),
            P("ep", None, "tp"),
            P("ep", None, "tp"),
            P("ep", None, "tp"),
        ),
        check_vma=False,
    )
```

```python
import functools
import math

import jax
import jax.numpy as jnp
from jax import lax
from jax.experimental import pallas as pl
from jax.experimental.pallas import tpu as pltpu
from jax.sharding import PartitionSpec as P


epsilon = 1e-06
f32 = jnp.float32
bf16 = jnp.bfloat16
VMEM = pl.BlockSpec(memory_space=pltpu.VMEM)
SMEM = pl.BlockSpec(memory_space=pltpu.SMEM)
HBM = pl.BlockSpec(memory_space=pltpu.HBM)
MIB = 1 << 20
LONG = pl.CostEstimate(flops=10**10, bytes_accessed=10**6, transcendentals=0)


def dot(left, right):
    return lax.dot_general(left, right, (((1,), (0,)), ((), ())), preferred_element_type=f32)


def dot_nt(left, right):
    return lax.dot_general(left, right, (((1,), (1,)), ((), ())), preferred_element_type=f32)


def silu(value):
    return value / (1.0 + jnp.exp(-value))


def sigmoid(value):
    return 1.0 / (1.0 + jnp.exp(-value))


def rms_rows(values, gain):
    return values * lax.rsqrt(jnp.mean(values * values, axis=-1, keepdims=True) + epsilon) * gain


def spread_heads(values, width):
    rows, heads = values.shape
    return jnp.concatenate(
        [jnp.broadcast_to(values[:, h : h + 1], (rows, width)) for h in range(heads)], axis=1
    )


def in_hbm(values):
    return pltpu.with_memory_space_constraint(values, pltpu.HBM)


def taps_first(values):
    return values.transpose(1, 0, 2)


def pack_kernel(gate_ref, up_ref, down_ref, ids_ref, weights_ref, out_ref, *, dests):
    rows, hidden = gate_ref.shape
    share = hidden // dests
    lanes = out_ref.shape[2]
    seqs, top_count = ids_ref.shape
    gate = gate_ref[...].astype(f32)
    up = up_ref[...].astype(f32)
    down = down_ref[...].astype(f32)
    ids = ids_ref[...]
    weights = weights_ref[...]
    expert = lax.broadcasted_iota(jnp.int32, (seqs, dests), 1)
    weight_of = jnp.zeros((seqs, dests), f32)
    for k in range(top_count):
        weight_of += jnp.where(ids[:, k : k + 1] == expert, weights[:, k : k + 1], 0.0)
    high = weight_of.astype(bf16).astype(f32)
    low = weight_of - high
    if rows > seqs:
        rest = jnp.zeros((rows - seqs, dests), f32)
        high = jnp.concatenate((high, rest), axis=0)
        low = jnp.concatenate((low, rest), axis=0)
    for j in range(dests):
        part = slice(j * share, (j + 1) * share)
        block = [gate[:, part], up[:, part], down[:, part], high[:, j : j + 1], low[:, j : j + 1]]
        spare = lanes - 3 * share - 2
        if spare:
            block.append(jnp.zeros((rows, spare), f32))
        out_ref[j] = jnp.concatenate(block, axis=1).astype(bf16)


def mixer_kernel(*refs, n_tp, held):
    tp_ref, w_x, w_b = refs[:3]
    sources = refs[3 : 3 + held]
    part_ref, conv_x_out, conv_b_out, conv_c_out, state_out = refs[3 + held : 8 + held]
    targets = refs[8 + held : 8 + 2 * held]
    in_sems, state_sems, out_sems = refs[8 + 2 * held :]
    (
        tokens_ref,
        gain_ref,
        w_dt_ref,
        dt_bias_ref,
        a_log_ref,
        d_skip_ref,
        taps_x_ref,
        taps_b_ref,
        taps_c_ref,
        group_gain_ref,
        conv_x_ref,
        conv_b_ref,
        conv_c_ref,
        w_c,
        w_z,
        w_out,
        state,
    ) = targets
    seqs, heads, head_dim, state_dim = state.shape
    channels = heads * head_dim
    groups = w_b.shape[1] // state_dim
    per_group = heads // groups
    width = channels // groups
    copy = pltpu.make_async_copy
    loads = [copy(sources[i], targets[i], in_sems.at[i]) for i in range(held - 1)]
    *small_loads, load_c, load_z, load_out = loads
    state_loads = [copy(sources[-1].at[s], state.at[s], state_sems.at[s]) for s in range(seqs)]
    stores = [copy(state.at[s], state_out.at[s], out_sems.at[s]) for s in range(seqs)]
    for load in [*small_loads, load_c, *state_loads, load_z, load_out]:
        load.start()
    for load in small_loads:
        load.wait()

    normed = rms_rows(tokens_ref[...].astype(f32), gain_ref[...]).astype(bf16)
    dt_all = dot_nt(normed, w_dt_ref[...])
    own = tp_ref[0]
    dt_raw = jnp.zeros((seqs, heads), f32)
    for i in range(n_tp):
        dt_raw += jnp.where(own == i, dt_all[:, i * heads : (i + 1) * heads], 0.0)
    shifted = dt_raw + dt_bias_ref[...]
    step = jnp.maximum(shifted, 0.0) + jnp.log1p(jnp.exp(-jnp.abs(shifted)))
    decay = jnp.exp(-step * jnp.exp(a_log_ref[...]))

    def short_conv(previous_ref, fresh, taps_ref, out_ref):
        taps = taps_ref[...].astype(f32)
        last = taps.shape[0] - 1
        total = fresh * taps[last:]
        for k in range(last):
            total += previous_ref[k].astype(f32) * taps[k : k + 1]
            out_ref[k] = previous_ref[k + 1] if k + 1 < last else fresh.astype(bf16)
        return silu(total)

    def projected(ref):
        return dot(normed, ref[...]).astype(bf16).astype(f32)

    xs = short_conv(conv_x_ref, projected(w_x), taps_x_ref, conv_x_out)
    bs = short_conv(conv_b_ref, projected(w_b), taps_b_ref, conv_b_out)
    load_c.wait()
    cs = short_conv(conv_c_ref, projected(w_c), taps_c_ref, conv_c_out).astype(bf16)
    scaled = (spread_heads(step, head_dim) * xs).T
    row = lax.broadcasted_iota(jnp.int32, (seqs, width), 0)
    readout = [jnp.zeros((seqs, width), f32) for _ in range(groups)]
    for s in range(seqs):
        state_loads[s].wait()
        for g in range(groups):
            key = bs[s : s + 1, g * state_dim : (g + 1) * state_dim]
            fresh = []
            for h in range(g * per_group, (g + 1) * per_group):
                column = scaled[h * head_dim : (h + 1) * head_dim, s : s + 1]
                updated = decay[s : s + 1, h : h + 1] * state[s, h] + column * key
                state[s, h] = updated
                fresh.append(updated.astype(bf16))
            read = dot_nt(
                cs[:, g * state_dim : (g + 1) * state_dim], jnp.concatenate(fresh, axis=0)
            )
            readout[g] = jnp.where(row == s, read, readout[g])
        stores[s].start()
    load_z.wait()
    z_gate = silu(projected(w_z))
    skip = spread_heads(d_skip_ref[...], head_dim) * xs
    mixed = []
    for g in range(groups):
        part = slice(g * width, (g + 1) * width)
        gated = (readout[g] + skip[:, part]) * z_gate[:, part]
        mixed.append(rms_rows(gated, group_gain_ref[:, part]).astype(bf16))
    load_out.wait()
    part_ref[...] = dot(jnp.concatenate(mixed, axis=1), w_out[...]).astype(bf16)
    for store in stores:
        store.wait()


def norm_kernel(tokens_ref, own_ref, other_ref, gain_ref, spread_ref, residual_ref):
    seqs = tokens_ref.shape[0]
    summed = own_ref[...].astype(f32) + other_ref[...].astype(f32)
    residual = (tokens_ref[...].astype(f32) + summed).astype(bf16)
    residual_ref[...] = residual
    normed = rms_rows(residual.astype(f32), gain_ref[...]).astype(bf16)
    for j in range(spread_ref.shape[0] // seqs):
        spread_ref[j * seqs : (j + 1) * seqs] = normed


def experts_kernel(
    rows_ref, packed_ref, gate_ref, up_ref, down_ref, branch_ref, out_ref, *, share, seqs, n_tp
):
    blocks, block_rows, lanes = packed_ref.shape
    count, model = rows_ref.shape
    rows = rows_ref[...]
    active = (silu(dot(rows, gate_ref[0])) * dot(rows, up_ref[0])).astype(bf16)
    routed = dot(active, down_ref[0])
    packed = packed_ref[...].reshape(blocks * block_rows, lanes)
    hidden = dot(rows, packed)
    lane = lax.broadcasted_iota(jnp.int32, (count, lanes), 1)
    dense = silu(pltpu.roll(hidden, 2 * share, 1)) * pltpu.roll(hidden, share, 1)
    chosen = (lane >= 2 * share) & (lane < 3 * share)
    dense = jnp.where(chosen, dense, 0.0).astype(bf16)
    dense_out = dot_nt(dense, packed)
    branch = sigmoid(
        jnp.sum(rows.astype(f32) * branch_ref[...].astype(f32), axis=1, keepdims=True)
    )
    table = jnp.concatenate(
        [packed_ref[i, :seqs].astype(f32) for i in range(blocks)], axis=0
    )
    weight = jnp.sum(
        jnp.where((lane >= 3 * share) & (lane < 3 * share + 2), table, 0.0), axis=1, keepdims=True
    )
    result = weight * routed + branch * dense_out
    half = model // n_tp
    for j in range(blocks):
        for q in range(n_tp):
            place = (j * n_tp + q) * seqs
            out_ref[place : place + seqs] = result[
                j * seqs : (j + 1) * seqs, q * half : (q + 1) * half
            ].astype(bf16)


def sum_kernel(tp_ref, parts_ref, residual_ref, out_ref, *, n_tp):
    seqs, half = out_ref.shape
    own = tp_ref[0]
    total = jnp.zeros((seqs, half), f32)
    for q in range(n_tp):
        total += jnp.where(
            own == q, residual_ref[:, q * half : (q + 1) * half].astype(f32), 0.0
        )
    for i in range(parts_ref.shape[0] // seqs):
        total += parts_ref[i * seqs : (i + 1) * seqs].astype(f32)
    out_ref[...] = total.astype(bf16)


def body(
    tokens,
    ssm_state,
    conv_x,
    conv_b,
    conv_c,
    w_x,
    w_z,
    w_b,
    w_c,
    w_dt,
    dt_bias,
    a_log,
    d_skip,
    taps_x,
    taps_b,
    taps_c,
    norm1_gain,
    group_gain,
    w_out,
    norm2_gain,
    route_ids,
    route_weights,
    exp_gate,
    exp_up,
    exp_down,
    dense_gate,
    dense_up,
    dense_down,
    branch_gate,
):
    seqs, model = tokens.shape
    n_ep = lax.axis_size("ep")
    n_tp = lax.axis_size("tp")
    tp_index = lax.axis_index("tp").astype(jnp.int32)[None]
    sds = jax.ShapeDtypeStruct

    rows, hidden = dense_gate.shape
    share = hidden // n_ep
    lanes = 128 * math.ceil((3 * share + 2) / 128)
    packed = pl.pallas_call(
        functools.partial(pack_kernel, dests=n_ep),
        out_shape=pltpu.HBM((n_ep, rows, lanes), bf16),
        in_specs=[VMEM] * 5,
        out_specs=VMEM,
        compiler_params=pltpu.CompilerParams(vmem_limit_bytes=4 * MIB),
        cost_estimate=LONG,
        name="pack",
    )(*map(in_hbm, (dense_gate, dense_up, dense_down.T, route_ids, route_weights)))
    packed = lax.all_to_all(packed, "ep", split_axis=0, concat_axis=0, tiled=True)

    held = (
        tokens,
        norm1_gain[None],
        w_dt.T,
        dt_bias[None],
        a_log[None],
        d_skip[None],
        taps_x,
        taps_b,
        taps_c,
        group_gain[None],
        taps_first(conv_x),
        taps_first(conv_b),
        taps_first(conv_c),
        w_c,
        w_z,
        w_out,
        ssm_state,
    )
    part, conv_x_next, conv_b_next, conv_c_next, state_next = pl.pallas_call(
        functools.partial(mixer_kernel, n_tp=n_tp, held=len(held)),
        out_shape=(
            sds((seqs, model), bf16),
            sds(taps_first(conv_x).shape, bf16),
            sds(taps_first(conv_b).shape, bf16),
            sds(taps_first(conv_c).shape, bf16),
            sds(ssm_state.shape, f32),
        ),
        in_specs=[SMEM] + [VMEM] * 2 + [HBM] * len(held),
        out_specs=(VMEM, VMEM, VMEM, VMEM, HBM),
        scratch_shapes=[pltpu.VMEM(value.shape, value.dtype) for value in held]
        + [
            pltpu.SemaphoreType.DMA((len(held) - 1,)),
            pltpu.SemaphoreType.DMA((seqs,)),
            pltpu.SemaphoreType.DMA((seqs,)),
        ],
        compiler_params=pltpu.CompilerParams(vmem_limit_bytes=20 * MIB),
        name="mixer",
    )(tp_index, w_x, w_b, *map(in_hbm, held))

    if n_tp == 2:
        other = lax.ppermute(part, "tp", [(0, 1), (1, 0)])
    else:
        gathered = lax.all_gather(part, "tp", axis=0).astype(f32)
        total = gathered[0]
        for i in range(1, n_tp):
            total = total + gathered[i]
        other = total - part.astype(f32)

    spread, residual = pl.pallas_call(
        norm_kernel,
        out_shape=(sds((n_ep * seqs, model), bf16), sds((seqs, model), bf16)),
        in_specs=[VMEM] * 4,
        out_specs=(VMEM, VMEM),
        compiler_params=pltpu.CompilerParams(vmem_limit_bytes=4 * MIB),
        cost_estimate=LONG,
        name="norm",
    )(tokens, part, other, norm2_gain[None])
    everyone = lax.all_to_all(spread, "ep", split_axis=0, concat_axis=0, tiled=True)

    outgoing = pl.pallas_call(
        functools.partial(experts_kernel, share=share, seqs=seqs, n_tp=n_tp),
        out_shape=sds((n_ep * n_tp * seqs, model // n_tp), bf16),
        in_specs=[VMEM] * 6,
        out_specs=VMEM,
        compiler_params=pltpu.CompilerParams(vmem_limit_bytes=12 * MIB),
        name="experts",
    )(everyone, packed, exp_gate, exp_up, exp_down, branch_gate[None])
    parts = lax.all_to_all(outgoing, ("ep", "tp"), split_axis=0, concat_axis=0, tiled=True)

    mixed = pl.pallas_call(
        functools.partial(sum_kernel, n_tp=n_tp),
        out_shape=sds((seqs, model // n_tp), bf16),
        in_specs=[SMEM, VMEM, VMEM],
        out_specs=VMEM,
        compiler_params=pltpu.CompilerParams(vmem_limit_bytes=4 * MIB),
        name="total",
    )(tp_index, parts, residual)
    return (
        mixed,
        state_next,
        taps_first(conv_x_next),
        taps_first(conv_b_next),
        taps_first(conv_c_next),
    )


def solution(mesh):
    return jax.shard_map(
        body,
        mesh=mesh,
        in_specs=(
            P("ep", None),
            P("ep", "tp", None, None),
            P("ep", None, "tp"),
            P("ep", None, "tp"),
            P("ep", None, "tp"),
            P(None, "tp"),
            P(None, "tp"),
            P(None, "tp"),
            P(None, "tp"),
            P(),
            P("tp"),
            P("tp"),
            P("tp"),
            P(None, "tp"),
            P(None, "tp"),
            P(None, "tp"),
            P(),
            P("tp"),
            P("tp", None),
            P(),
            P("ep", None),
            P("ep", None),
            P("ep", None, "tp"),
            P("ep", None, "tp"),
            P("ep", "tp", None),
            P("ep", "tp"),
            P("ep", "tp"),
            P("tp", "ep"),
            P(),
        ),
        out_specs=(
            P("ep", "tp"),
            P("ep", "tp", None, None),
            P("ep", None, "tp"),
            P("ep", None, "tp"),
            P("ep", None, "tp"),
        ),
        check_vma=False,
    )
```

```python
import functools
import math

import jax
import jax.numpy as jnp
from jax import lax
from jax.experimental import pallas as pl
from jax.experimental.pallas import tpu as pltpu
from jax.sharding import PartitionSpec as P


epsilon = 1e-06
f32 = jnp.float32
bf16 = jnp.bfloat16
VMEM = pl.BlockSpec(memory_space=pltpu.VMEM)
SMEM = pl.BlockSpec(memory_space=pltpu.SMEM)
HBM = pl.BlockSpec(memory_space=pltpu.HBM)
MIB = 1 << 20
LONG = pl.CostEstimate(flops=10**10, bytes_accessed=10**6, transcendentals=0)


def dot(left, right):
    return lax.dot_general(left, right, (((1,), (0,)), ((), ())), preferred_element_type=f32)


def dot_nt(left, right):
    return lax.dot_general(left, right, (((1,), (1,)), ((), ())), preferred_element_type=f32)


def silu(value):
    return value / (1.0 + jnp.exp(-value))


def sigmoid(value):
    return 1.0 / (1.0 + jnp.exp(-value))


def rms_rows(values, gain):
    return values * lax.rsqrt(jnp.mean(values * values, axis=-1, keepdims=True) + epsilon) * gain


def spread_heads(values, width):
    rows, heads = values.shape
    return jnp.concatenate(
        [jnp.broadcast_to(values[:, h : h + 1], (rows, width)) for h in range(heads)], axis=1
    )


def in_hbm(values):
    return pltpu.with_memory_space_constraint(values, pltpu.HBM)


def taps_first(values):
    return values.transpose(1, 0, 2)


def pack_kernel(gate_ref, up_ref, down_ref, ids_ref, weights_ref, out_ref, *, dests):
    rows, hidden = gate_ref.shape
    share = hidden // dests
    lanes = out_ref.shape[2]
    seqs, top_count = ids_ref.shape
    gate = gate_ref[...].astype(f32)
    up = up_ref[...].astype(f32)
    down = down_ref[...].astype(f32)
    ids = ids_ref[...]
    weights = weights_ref[...]
    expert = lax.broadcasted_iota(jnp.int32, (seqs, dests), 1)
    weight_of = jnp.zeros((seqs, dests), f32)
    for k in range(top_count):
        weight_of += jnp.where(ids[:, k : k + 1] == expert, weights[:, k : k + 1], 0.0)
    high = weight_of.astype(bf16).astype(f32)
    low = weight_of - high
    if rows > seqs:
        rest = jnp.zeros((rows - seqs, dests), f32)
        high = jnp.concatenate((high, rest), axis=0)
        low = jnp.concatenate((low, rest), axis=0)
    for j in range(dests):
        part = slice(j * share, (j + 1) * share)
        block = [gate[:, part], up[:, part], down[:, part], high[:, j : j + 1], low[:, j : j + 1]]
        spare = lanes - 3 * share - 2
        if spare:
            block.append(jnp.zeros((rows, spare), f32))
        out_ref[j] = jnp.concatenate(block, axis=1).astype(bf16)


def mixer_kernel(*refs, n_tp, held):
    tp_ref, w_x, w_b = refs[:3]
    sources = refs[3 : 3 + held]
    part_ref, scaled_ref, key_ref, decay_ref = refs[3 + held : 7 + held]
    conv_outs = refs[7 + held : 10 + held]
    targets = refs[10 + held : 10 + 2 * held]
    conv_x_next, conv_b_next, conv_c_next = conv_next = refs[10 + 2 * held : 13 + 2 * held]
    in_sems, state_sems, out_sems = refs[13 + 2 * held :]
    (
        tokens_ref,
        gain_ref,
        w_dt_ref,
        dt_bias_ref,
        a_log_ref,
        d_skip_ref,
        taps_x_ref,
        taps_b_ref,
        taps_c_ref,
        group_gain_ref,
        conv_x_ref,
        conv_b_ref,
        conv_c_ref,
        w_c,
        w_z,
        w_out,
        state,
    ) = targets
    seqs, heads, head_dim, state_dim = state.shape
    channels = heads * head_dim
    groups = w_b.shape[1] // state_dim
    per_group = heads // groups
    width = channels // groups
    copy = pltpu.make_async_copy
    loads = [copy(sources[i], targets[i], in_sems.at[i]) for i in range(held - 1)]
    *small_loads, load_c, load_z, load_out = loads
    state_loads = [copy(sources[-1].at[s], state.at[s], state_sems.at[s]) for s in range(seqs)]
    stores = [copy(conv_next[i], conv_outs[i], out_sems.at[i]) for i in range(3)]
    for load in [*small_loads, load_c, *state_loads, load_z, load_out]:
        load.start()
    for load in small_loads:
        load.wait()

    normed = rms_rows(tokens_ref[...].astype(f32), gain_ref[...]).astype(bf16)
    dt_all = dot_nt(normed, w_dt_ref[...])
    own = tp_ref[0]
    dt_raw = jnp.zeros((seqs, heads), f32)
    for i in range(n_tp):
        dt_raw += jnp.where(own == i, dt_all[:, i * heads : (i + 1) * heads], 0.0)
    shifted = dt_raw + dt_bias_ref[...]
    step = jnp.maximum(shifted, 0.0) + jnp.log1p(jnp.exp(-jnp.abs(shifted)))
    decay = jnp.exp(-step * jnp.exp(a_log_ref[...]))

    def short_conv(previous_ref, fresh, taps_ref, out_ref):
        taps = taps_ref[...].astype(f32)
        last = taps.shape[0] - 1
        total = fresh * taps[last:]
        for k in range(last):
            total += previous_ref[k].astype(f32) * taps[k : k + 1]
            out_ref[k] = previous_ref[k + 1] if k + 1 < last else fresh.astype(bf16)
        return silu(total)

    def projected(ref):
        return dot(normed, ref[...]).astype(bf16).astype(f32)

    xs = short_conv(conv_x_ref, projected(w_x), taps_x_ref, conv_x_next)
    bs = short_conv(conv_b_ref, projected(w_b), taps_b_ref, conv_b_next)
    load_c.wait()
    cs = short_conv(conv_c_ref, projected(w_c), taps_c_ref, conv_c_next)
    for store in stores:
        store.start()
    queries = cs.astype(bf16)
    scaled = spread_heads(step, head_dim) * xs
    scaled_ref[...] = scaled
    key_ref[...] = bs
    decay_ref[...] = decay
    row = lax.broadcasted_iota(jnp.int32, (seqs, width), 0)
    readout = [jnp.zeros((seqs, width), f32) for _ in range(groups)]
    for s in range(seqs):
        state_loads[s].wait()
        for g in range(groups):
            block = state[s, g * per_group : (g + 1) * per_group].reshape(width, state_dim)
            read = dot_nt(queries[:, g * state_dim : (g + 1) * state_dim], block.astype(bf16))
            readout[g] = jnp.where(row == s, read, readout[g])
    load_z.wait()
    z_gate = silu(projected(w_z))
    skip = spread_heads(d_skip_ref[...], head_dim) * xs
    kept = spread_heads(decay, head_dim)
    mixed = []
    for g in range(groups):
        part = slice(g * width, (g + 1) * width)
        own = slice(g * state_dim, (g + 1) * state_dim)
        match = jnp.sum(bs[:, own] * cs[:, own], axis=1, keepdims=True)
        read = kept[:, part] * readout[g] + scaled[:, part] * match
        gated = (read + skip[:, part]) * z_gate[:, part]
        mixed.append(rms_rows(gated, group_gain_ref[:, part]).astype(bf16))
    load_out.wait()
    part_ref[...] = dot(jnp.concatenate(mixed, axis=1), w_out[...]).astype(bf16)
    for store in stores:
        store.wait()


def advance_kernel(
    scaled_ref, key_ref, decay_ref, state_hbm, state_out, state, in_sems, out_sems
):
    seqs, heads, head_dim, state_dim = state.shape
    per_group = heads * state_dim // key_ref.shape[1]
    copy = pltpu.make_async_copy
    loads = [copy(state_hbm.at[s], state.at[s], in_sems.at[s]) for s in range(seqs)]
    stores = [copy(state.at[s], state_out.at[s], out_sems.at[s]) for s in range(seqs)]
    for load in loads:
        load.start()
    scaled = scaled_ref[...].T
    keys = key_ref[...]
    decay = decay_ref[...]
    for s in range(seqs):
        loads[s].wait()
        for h in range(heads):
            g = h // per_group
            key = keys[s : s + 1, g * state_dim : (g + 1) * state_dim]
            column = scaled[h * head_dim : (h + 1) * head_dim, s : s + 1]
            state[s, h] = decay[s : s + 1, h : h + 1] * state[s, h] + column * key
        stores[s].start()
    for store in stores:
        store.wait()


def norm_kernel(tokens_ref, own_ref, other_ref, gain_ref, spread_ref, residual_ref):
    seqs = tokens_ref.shape[0]
    summed = own_ref[...].astype(f32) + other_ref[...].astype(f32)
    residual = (tokens_ref[...].astype(f32) + summed).astype(bf16)
    residual_ref[...] = residual
    normed = rms_rows(residual.astype(f32), gain_ref[...]).astype(bf16)
    for j in range(spread_ref.shape[0] // seqs):
        spread_ref[j * seqs : (j + 1) * seqs] = normed


def experts_kernel(
    core_ref,
    own_ref,
    other_ref,
    packed_ref,
    gate_ref,
    up_ref,
    down_ref,
    branch_ref,
    keep_ref,
    send_ref,
    *,
    share,
    seqs,
    n_tp,
):
    blocks, block_rows, lanes = packed_ref.shape
    core = core_ref[0]
    half_count, model = own_ref.shape
    count = 2 * half_count
    rows = jnp.concatenate((own_ref[...], other_ref[...]), axis=0)
    active = (silu(dot(rows, gate_ref[0])) * dot(rows, up_ref[0])).astype(bf16)
    routed = dot(active, down_ref[0])
    packed = packed_ref[...].reshape(blocks * block_rows, lanes)
    hidden = dot(rows, packed)
    lane = lax.broadcasted_iota(jnp.int32, (count, lanes), 1)
    dense = silu(pltpu.roll(hidden, 2 * share, 1)) * pltpu.roll(hidden, share, 1)
    chosen = (lane >= 2 * share) & (lane < 3 * share)
    dense = jnp.where(chosen, dense, 0.0).astype(bf16)
    dense_out = dot_nt(dense, packed)
    branch = sigmoid(
        jnp.sum(rows.astype(f32) * branch_ref[...].astype(f32)[None], axis=1, keepdims=True)
    )
    table = jnp.concatenate(
        [
            packed_ref[2 * i + place, :seqs].astype(f32)
            for place in (core, 1 - core)
            for i in range(blocks // 2)
        ],
        axis=0,
    )
    weight = jnp.sum(
        jnp.where((lane >= 3 * share) & (lane < 3 * share + 2), table, 0.0), axis=1, keepdims=True
    )
    result = weight * routed + branch * dense_out
    half = model // n_tp
    for i in range(blocks // 2):
        for q in range(n_tp):
            place = (i * n_tp + q) * seqs
            part = slice(q * half, (q + 1) * half)
            keep_ref[place : place + seqs] = result[i * seqs : (i + 1) * seqs, part]
            send_ref[place : place + seqs] = result[
                half_count + i * seqs : half_count + (i + 1) * seqs, part
            ].astype(bf16)


def add_kernel(left_ref, right_ref, out_ref):
    out_ref[...] = (left_ref[...] + right_ref[...].astype(f32)).astype(bf16)


def sum_kernel(tp_ref, parts_ref, residual_ref, out_ref, *, n_tp):
    seqs, half = out_ref.shape
    own = tp_ref[0]
    total = jnp.zeros((seqs, half), f32)
    for q in range(n_tp):
        total += jnp.where(
            own == q, residual_ref[:, q * half : (q + 1) * half].astype(f32), 0.0
        )
    for i in range(parts_ref.shape[0] // seqs):
        total += parts_ref[i * seqs : (i + 1) * seqs].astype(f32)
    out_ref[...] = total.astype(bf16)


def body(
    tokens,
    ssm_state,
    conv_x,
    conv_b,
    conv_c,
    w_x,
    w_z,
    w_b,
    w_c,
    w_dt,
    dt_bias,
    a_log,
    d_skip,
    taps_x,
    taps_b,
    taps_c,
    norm1_gain,
    group_gain,
    w_out,
    norm2_gain,
    route_ids,
    route_weights,
    exp_gate,
    exp_up,
    exp_down,
    dense_gate,
    dense_up,
    dense_down,
    branch_gate,
):
    seqs, model = tokens.shape
    n_ep = lax.axis_size("ep")
    n_tp = lax.axis_size("tp")
    core_index = (lax.axis_index("ep").astype(jnp.int32) % 2)[None]
    tp_index = lax.axis_index("tp").astype(jnp.int32)[None]
    sds = jax.ShapeDtypeStruct

    rows, hidden = dense_gate.shape
    share = hidden // n_ep
    lanes = 128 * math.ceil((3 * share + 2) / 128)
    packed = pl.pallas_call(
        functools.partial(pack_kernel, dests=n_ep),
        out_shape=pltpu.HBM((n_ep, rows, lanes), bf16),
        in_specs=[VMEM] * 5,
        out_specs=VMEM,
        compiler_params=pltpu.CompilerParams(vmem_limit_bytes=4 * MIB),
        cost_estimate=LONG,
        name="pack",
    )(*map(in_hbm, (dense_gate, dense_up, dense_down.T, route_ids, route_weights)))
    packed = lax.all_to_all(packed, "ep", split_axis=0, concat_axis=0, tiled=True)

    held = (
        tokens,
        norm1_gain[None],
        w_dt.T,
        dt_bias[None],
        a_log[None],
        d_skip[None],
        taps_x,
        taps_b,
        taps_c,
        group_gain[None],
        taps_first(conv_x),
        taps_first(conv_b),
        taps_first(conv_c),
        w_c,
        w_z,
        w_out,
        ssm_state,
    )
    part, scaled, keys, decay, conv_x_next, conv_b_next, conv_c_next = pl.pallas_call(
        functools.partial(mixer_kernel, n_tp=n_tp, held=len(held)),
        out_shape=(
            sds((seqs, model), bf16),
            sds((seqs, w_x.shape[1]), f32),
            sds((seqs, w_b.shape[1]), f32),
            sds((seqs, ssm_state.shape[1]), f32),
            *[sds(taps_first(value).shape, bf16) for value in (conv_x, conv_b, conv_c)],
        ),
        in_specs=[SMEM] + [VMEM] * 2 + [HBM] * len(held),
        out_specs=(VMEM,) * 4 + (HBM,) * 3,
        scratch_shapes=[pltpu.VMEM(value.shape, value.dtype) for value in held]
        + [pltpu.VMEM(taps_first(value).shape, bf16) for value in (conv_x, conv_b, conv_c)]
        + [
            pltpu.SemaphoreType.DMA((len(held) - 1,)),
            pltpu.SemaphoreType.DMA((seqs,)),
            pltpu.SemaphoreType.DMA((3,)),
        ],
        compiler_params=pltpu.CompilerParams(vmem_limit_bytes=20 * MIB),
        name="mixer",
    )(tp_index, w_x, w_b, *map(in_hbm, held))

    state_next = pl.pallas_call(
        advance_kernel,
        out_shape=sds(ssm_state.shape, f32),
        in_specs=[VMEM] * 3 + [HBM],
        out_specs=HBM,
        scratch_shapes=[
            pltpu.VMEM(ssm_state.shape, f32),
            pltpu.SemaphoreType.DMA((seqs,)),
            pltpu.SemaphoreType.DMA((seqs,)),
        ],
        compiler_params=pltpu.CompilerParams(vmem_limit_bytes=12 * MIB),
        name="advance",
    )(scaled, keys, decay, in_hbm(ssm_state))

    if n_tp == 2:
        other = lax.ppermute(part, "tp", [(0, 1), (1, 0)])
    else:
        gathered = lax.all_gather(part, "tp", axis=0).astype(f32)
        total = gathered[0]
        for i in range(1, n_tp):
            total = total + gathered[i]
        other = total - part.astype(f32)

    spread, residual = pl.pallas_call(
        norm_kernel,
        out_shape=(sds((n_ep // 2 * seqs, model), bf16), sds((seqs, model), bf16)),
        in_specs=[VMEM] * 4,
        out_specs=(VMEM, VMEM),
        compiler_params=pltpu.CompilerParams(vmem_limit_bytes=4 * MIB),
        cost_estimate=LONG,
        name="norm",
    )(tokens, part, other, norm2_gain[None])
    groups = [[2 * chip + core for chip in range(n_ep // 2)] for core in range(2)]
    swap = [(i, i ^ 1) for i in range(n_ep)]
    own_core = lax.all_to_all(
        spread, "ep", split_axis=0, concat_axis=0, tiled=True, axis_index_groups=groups
    )
    other_core = lax.ppermute(own_core, "ep", swap)

    blocks = (n_ep // 2 * n_tp * seqs, model // n_tp)
    keep, send = pl.pallas_call(
        functools.partial(experts_kernel, share=share, seqs=seqs, n_tp=n_tp),
        out_shape=(sds(blocks, f32), sds(blocks, bf16)),
        in_specs=[SMEM] + [VMEM] * 7,
        out_specs=(VMEM, VMEM),
        compiler_params=pltpu.CompilerParams(vmem_limit_bytes=12 * MIB),
        name="experts",
    )(core_index, own_core, other_core, packed, exp_gate, exp_up, exp_down, branch_gate)
    outgoing = pl.pallas_call(
        add_kernel,
        out_shape=sds(blocks, bf16),
        in_specs=[VMEM] * 2,
        out_specs=VMEM,
        compiler_params=pltpu.CompilerParams(vmem_limit_bytes=4 * MIB),
        name="add",
    )(keep, lax.ppermute(send, "ep", swap))
    flat_groups = [[ep * n_tp + q for ep in group for q in range(n_tp)] for group in groups]
    parts = lax.all_to_all(
        outgoing,
        ("ep", "tp"),
        split_axis=0,
        concat_axis=0,
        tiled=True,
        axis_index_groups=flat_groups,
    )

    mixed = pl.pallas_call(
        functools.partial(sum_kernel, n_tp=n_tp),
        out_shape=sds((seqs, model // n_tp), bf16),
        in_specs=[SMEM, VMEM, VMEM],
        out_specs=VMEM,
        compiler_params=pltpu.CompilerParams(vmem_limit_bytes=4 * MIB),
        name="total",
    )(tp_index, parts, residual)
    return (
        mixed,
        state_next,
        taps_first(conv_x_next),
        taps_first(conv_b_next),
        taps_first(conv_c_next),
    )


def solution(mesh):
    return jax.shard_map(
        body,
        mesh=mesh,
        in_specs=(
            P("ep", None),
            P("ep", "tp", None, None),
            P("ep", None, "tp"),
            P("ep", None, "tp"),
            P("ep", None, "tp"),
            P(None, "tp"),
            P(None, "tp"),
            P(None, "tp"),
            P(None, "tp"),
            P(),
            P("tp"),
            P("tp"),
            P("tp"),
            P(None, "tp"),
            P(None, "tp"),
            P(None, "tp"),
            P(),
            P("tp"),
            P("tp", None),
            P(),
            P("ep", None),
            P("ep", None),
            P("ep", None, "tp"),
            P("ep", None, "tp"),
            P("ep", "tp", None),
            P("ep", "tp"),
            P("ep", "tp"),
            P("tp", "ep"),
            P(),
        ),
        out_specs=(
            P("ep", "tp"),
            P("ep", "tp", None, None),
            P("ep", None, "tp"),
            P("ep", None, "tp"),
            P("ep", None, "tp"),
        ),
        check_vma=False,
    )
```

```python
import functools

import jax
import jax.numpy as jnp
from jax import lax
from jax.experimental import pallas as pl
from jax.experimental.pallas import tpu as pltpu
from jax.sharding import PartitionSpec as P


epsilon = 1e-06
f32 = jnp.float32
bf16 = jnp.bfloat16
VMEM = pl.BlockSpec(memory_space=pltpu.VMEM)
SMEM = pl.BlockSpec(memory_space=pltpu.SMEM)
HBM = pl.BlockSpec(memory_space=pltpu.HBM)
MIB = 1 << 20
LANES = 128


def dot(left, right):
    return lax.dot_general(left, right, (((1,), (0,)), ((), ())), preferred_element_type=f32)


def dot_nt(left, right):
    return lax.dot_general(left, right, (((1,), (1,)), ((), ())), preferred_element_type=f32)


def silu(value):
    return value / (1.0 + jnp.exp(-value))


def sigmoid(value):
    return 1.0 / (1.0 + jnp.exp(-value))


def rms_rows(values, gain):
    return values * lax.rsqrt(jnp.mean(values * values, axis=-1, keepdims=True) + epsilon) * gain


def spread_heads(values, width):
    rows, heads = values.shape
    return jnp.concatenate(
        [jnp.broadcast_to(values[:, h : h + 1], (rows, width)) for h in range(heads)], axis=1
    )


def in_hbm(values):
    return pltpu.with_memory_space_constraint(values, pltpu.HBM)


def taps_first(values):
    return values.transpose(1, 0, 2)


def fold_of(rows, share):
    fold = 1
    while 4 * fold * share <= LANES and rows % (32 * fold) == 0:
        fold *= 2
    return fold


def packed_rows(rows, share, seqs):
    fold = fold_of(rows, share)
    return rows // fold + rows // (2 * fold) + seqs


def side_by_side(values, fold):
    rows, width = values.shape
    count, stride = rows // fold, LANES // fold
    pieces = []
    for k in range(fold):
        pieces.append(values[k * count : (k + 1) * count])
        if stride > width:
            pieces.append(jnp.zeros((count, stride - width), f32))
    return jnp.concatenate(pieces, axis=1)


def pack(gate, up, down, ids, weights, dest, fold):
    seqs, _ = ids.shape
    weight = jnp.sum(jnp.where(ids == dest, weights, 0.0), axis=1, keepdims=True)
    high = weight.astype(bf16).astype(f32)
    tail = jnp.concatenate((high, weight - high, jnp.zeros((seqs, LANES - 2), f32)), axis=1)
    both = side_by_side(jnp.concatenate((gate, up), axis=1), fold)
    return jnp.concatenate((both, side_by_side(down, 2 * fold), tail), axis=0)


def mixer_kernel(*refs, n_tp, held):
    place_ref = refs[0]
    sources = refs[1 : 1 + held]
    part_ref, scaled_ref, key_ref, decay_ref, own_ref, other_ref = refs[1 + held : 7 + held]
    conv_outs = refs[7 + held : 10 + held]
    targets = refs[10 + held : 10 + 2 * held]
    conv_x_next, conv_b_next, conv_c_next = conv_next = refs[10 + 2 * held : 13 + 2 * held]
    in_sems, state_sems, out_sems = refs[13 + 2 * held :]
    (
        tokens_ref,
        gain_ref,
        w_dt_ref,
        dt_bias_ref,
        a_log_ref,
        d_skip_ref,
        taps_x_ref,
        taps_b_ref,
        taps_c_ref,
        group_gain_ref,
        conv_x_ref,
        conv_b_ref,
        conv_c_ref,
        gate_ref,
        up_ref,
        down_ref,
        ids_ref,
        weights_ref,
        w_x,
        w_b,
        w_c,
        w_z,
        w_out,
        state,
    ) = targets
    seqs, heads, head_dim, state_dim = state.shape
    channels = heads * head_dim
    groups = w_b.shape[1] // state_dim
    per_group = heads // groups
    width = channels // groups
    copy = pltpu.make_async_copy
    loads = [copy(sources[i], targets[i], in_sems.at[i]) for i in range(held - 1)]
    *small_loads, load_x, load_b, load_c, load_z, load_out = loads
    state_loads = [copy(sources[-1].at[s], state.at[s], state_sems.at[s]) for s in range(seqs)]
    stores = [copy(conv_next[i], conv_outs[i], out_sems.at[i]) for i in range(3)]
    for load in [*small_loads, load_x, load_b, load_c, *state_loads, load_z, load_out]:
        load.start()
    for load in small_loads:
        load.wait()

    normed = rms_rows(tokens_ref[...].astype(f32), gain_ref[...]).astype(bf16)
    dt_all = dot_nt(normed, w_dt_ref[...])
    own = place_ref[0]
    dt_raw = jnp.zeros((seqs, heads), f32)
    for i in range(n_tp):
        dt_raw += jnp.where(own == i, dt_all[:, i * heads : (i + 1) * heads], 0.0)
    shifted = dt_raw + dt_bias_ref[...]
    step = jnp.maximum(shifted, 0.0) + jnp.log1p(jnp.exp(-jnp.abs(shifted)))
    decay = jnp.exp(-step * jnp.exp(a_log_ref[...]))

    first = place_ref[1] == 0
    gate = gate_ref[...].astype(f32)
    up = up_ref[...].astype(f32)
    down = down_ref[...].astype(f32)
    ids = ids_ref[...]
    weights = weights_ref[...]
    share = gate.shape[1] // (2 * own_ref.shape[0])
    fold = fold_of(gate.shape[0], share)
    for chip in range(own_ref.shape[0]):
        even, odd = [
            pack(*[value[:, j * share : (j + 1) * share] for value in (gate, up, down)], ids, weights, j, fold)
            for j in (2 * chip, 2 * chip + 1)
        ]
        own_ref[chip] = jnp.where(first, even, odd).astype(bf16)
        other_ref[chip] = jnp.where(first, odd, even).astype(bf16)

    def short_conv(previous_ref, fresh, taps_ref, out_ref):
        taps = taps_ref[...].astype(f32)
        last = taps.shape[0] - 1
        total = fresh * taps[last:]
        for k in range(last):
            total += previous_ref[k].astype(f32) * taps[k : k + 1]
            out_ref[k] = previous_ref[k + 1] if k + 1 < last else fresh.astype(bf16)
        return silu(total)

    def projected(ref):
        return dot(normed, ref[...]).astype(bf16).astype(f32)

    load_x.wait()
    xs = short_conv(conv_x_ref, projected(w_x), taps_x_ref, conv_x_next)
    load_b.wait()
    bs = short_conv(conv_b_ref, projected(w_b), taps_b_ref, conv_b_next)
    load_c.wait()
    cs = short_conv(conv_c_ref, projected(w_c), taps_c_ref, conv_c_next)
    for store in stores:
        store.start()
    queries = cs.astype(bf16)
    scaled = spread_heads(step, head_dim) * xs
    scaled_ref[...] = scaled
    key_ref[...] = bs
    decay_ref[...] = decay
    row = lax.broadcasted_iota(jnp.int32, (seqs, width), 0)
    readout = [jnp.zeros((seqs, width), f32) for _ in range(groups)]
    for s in range(seqs):
        state_loads[s].wait()
        for g in range(groups):
            block = state[s, g * per_group : (g + 1) * per_group].reshape(width, state_dim)
            read = dot_nt(queries[:, g * state_dim : (g + 1) * state_dim], block.astype(bf16))
            readout[g] = jnp.where(row == s, read, readout[g])
    load_z.wait()
    z_gate = silu(projected(w_z))
    skip = spread_heads(d_skip_ref[...], head_dim) * xs
    kept = spread_heads(decay, head_dim)
    mixed = []
    for g in range(groups):
        part = slice(g * width, (g + 1) * width)
        own = slice(g * state_dim, (g + 1) * state_dim)
        match = jnp.sum(bs[:, own] * cs[:, own], axis=1, keepdims=True)
        read = kept[:, part] * readout[g] + scaled[:, part] * match
        gated = (read + skip[:, part]) * z_gate[:, part]
        mixed.append(rms_rows(gated, group_gain_ref[:, part]).astype(bf16))
    load_out.wait()
    part_ref[...] = dot(jnp.concatenate(mixed, axis=1), w_out[...]).astype(bf16)
    for store in stores:
        store.wait()


def advance_kernel(
    scaled_ref, key_ref, decay_ref, state_hbm, state_out, state, in_sems, out_sems
):
    seqs, heads, head_dim, state_dim = state.shape
    per_group = heads * state_dim // key_ref.shape[1]
    copy = pltpu.make_async_copy
    loads = [copy(state_hbm.at[s], state.at[s], in_sems.at[s]) for s in range(seqs)]
    stores = [copy(state.at[s], state_out.at[s], out_sems.at[s]) for s in range(seqs)]
    for load in loads:
        load.start()
    scaled = scaled_ref[...].T
    keys = key_ref[...]
    decay = decay_ref[...]
    for s in range(seqs):
        loads[s].wait()
        for h in range(heads):
            g = h // per_group
            key = keys[s : s + 1, g * state_dim : (g + 1) * state_dim]
            column = scaled[h * head_dim : (h + 1) * head_dim, s : s + 1]
            state[s, h] = decay[s : s + 1, h : h + 1] * state[s, h] + column * key
        stores[s].start()
    for store in stores:
        store.wait()


def norm_kernel(
    tokens_ref, own_ref, other_ref, gain_ref, kept_ref, swapped_ref, spread_ref, residual_ref
):
    _, model = tokens_ref.shape
    chips, block, _ = kept_ref.shape
    summed = own_ref[...].astype(f32) + other_ref[...].astype(f32)
    residual = (tokens_ref[...].astype(f32) + summed).astype(bf16)
    residual_ref[...] = residual
    normed = rms_rows(residual.astype(f32), gain_ref[...])
    tiles = jnp.concatenate(
        [normed[:, k * LANES : (k + 1) * LANES] for k in range(model // LANES)], axis=0
    ).astype(bf16)
    count = tiles.shape[0]
    for chip in range(chips):
        spread_ref[chip, :count] = tiles
        spread_ref[chip, count : count + block] = kept_ref[chip]
        spread_ref[chip, count + block :] = swapped_ref[chip]


def token_rows(tiles_ref, seqs, model):
    rows = []
    for chip in range(tiles_ref.shape[0]):
        tiles = tiles_ref[chip, : seqs * model // LANES]
        rows.append(
            jnp.concatenate(
                [tiles[k * seqs : (k + 1) * seqs] for k in range(model // LANES)], axis=1
            )
        )
    return jnp.concatenate(rows, axis=0)


def branches(rows, table, gate_ref, up_ref, down_ref, branch_ref, wide, back, share):
    active = (silu(dot(rows, gate_ref[0])) * dot(rows, up_ref[0])).astype(bf16)
    routed = dot(active, down_ref[0])
    hidden = dot(rows, wide)
    lane = lax.broadcasted_iota(jnp.int32, hidden.shape, 1)
    dense = silu(hidden) * pltpu.roll(hidden, LANES - share, 1)
    dense = jnp.where(lane < share, dense, 0.0).astype(bf16)
    dense_out = dot_nt(dense, back)
    branch = sigmoid(
        jnp.sum(rows.astype(f32) * branch_ref[...].astype(f32)[None], axis=1, keepdims=True)
    )
    weight = jnp.sum(jnp.where(lane < 2, table, 0.0), axis=1, keepdims=True)
    return weight * routed + branch * dense_out


def store_parts(out_ref, result, seqs, n_tp):
    half = result.shape[1] // n_tp
    for i in range(result.shape[0] // seqs):
        for q in range(n_tp):
            place = (i * n_tp + q) * seqs
            value = result[i * seqs : (i + 1) * seqs, q * half : (q + 1) * half]
            out_ref[place : place + seqs] = value.astype(out_ref.dtype)


def own_experts_kernel(
    place_ref,
    got_ref,
    gate_ref,
    up_ref,
    down_ref,
    branch_ref,
    keep_ref,
    wide_ref,
    back_ref,
    table_ref,
    *,
    share,
    seqs,
    n_tp,
):
    model = wide_ref.shape[0]
    chips, total, _ = got_ref.shape
    rows = model // (2 * chips)
    count = seqs * model // LANES
    block = (total - count) // 2
    fold = fold_of(rows, share)
    core = place_ref[1]
    wide_rows, back_rows = rows // fold, rows // (2 * fold)
    for chip in range(chips):
        for parity in range(2):
            start = count + jnp.where(core == parity, 0, block)
            start = pl.multiple_of(start, 8)
            source = (2 * chip + parity) * rows
            wide = got_ref[chip, pl.ds(start, wide_rows)].astype(f32)
            for k in range(fold):
                moved = pltpu.roll(wide, (LANES - k * LANES // fold) % LANES, 1) if k else wide
                place = source + k * wide_rows
                wide_ref[place : place + wide_rows] = moved.astype(bf16)
            back = got_ref[chip, pl.ds(pl.multiple_of(start + wide_rows, 8), back_rows)].astype(f32)
            for k in range(2 * fold):
                moved = pltpu.roll(back, LANES - k * LANES // (2 * fold), 1) if k else back
                place = source + k * back_rows
                back_ref[place : place + back_rows] = moved.astype(bf16)
    tail = count + block - seqs
    table = jnp.concatenate([got_ref[i, tail : tail + seqs].astype(f32) for i in range(chips)], axis=0)
    table_ref[...] = jnp.concatenate(
        [got_ref[i, total - seqs :].astype(f32) for i in range(chips)], axis=0
    )
    result = branches(
        token_rows(got_ref, seqs, model),
        table,
        gate_ref,
        up_ref,
        down_ref,
        branch_ref,
        wide_ref[...],
        back_ref[...],
        share,
    )
    store_parts(keep_ref, result, seqs, n_tp)


def other_experts_kernel(
    got_ref,
    gate_ref,
    up_ref,
    down_ref,
    branch_ref,
    wide_ref,
    back_ref,
    table_ref,
    send_ref,
    *,
    share,
    seqs,
    n_tp,
):
    result = branches(
        token_rows(got_ref, seqs, wide_ref.shape[0]),
        table_ref[...],
        gate_ref,
        up_ref,
        down_ref,
        branch_ref,
        wide_ref[...],
        back_ref[...],
        share,
    )
    store_parts(send_ref, result, seqs, n_tp)


def add_kernel(left_ref, right_ref, out_ref):
    out_ref[...] = (left_ref[...] + right_ref[...].astype(f32)).astype(bf16)


def sum_kernel(tp_ref, parts_ref, residual_ref, out_ref, *, n_tp):
    seqs, half = out_ref.shape
    own = tp_ref[0]
    total = jnp.zeros((seqs, half), f32)
    for q in range(n_tp):
        total += jnp.where(
            own == q, residual_ref[:, q * half : (q + 1) * half].astype(f32), 0.0
        )
    for i in range(parts_ref.shape[0] // seqs):
        total += parts_ref[i * seqs : (i + 1) * seqs].astype(f32)
    out_ref[...] = total.astype(bf16)


def body(
    tokens,
    ssm_state,
    conv_x,
    conv_b,
    conv_c,
    w_x,
    w_z,
    w_b,
    w_c,
    w_dt,
    dt_bias,
    a_log,
    d_skip,
    taps_x,
    taps_b,
    taps_c,
    norm1_gain,
    group_gain,
    w_out,
    norm2_gain,
    route_ids,
    route_weights,
    exp_gate,
    exp_up,
    exp_down,
    dense_gate,
    dense_up,
    dense_down,
    branch_gate,
):
    seqs, model = tokens.shape
    n_ep = lax.axis_size("ep")
    n_tp = lax.axis_size("tp")
    place = jnp.stack((lax.axis_index("tp"), lax.axis_index("ep") % 2)).astype(jnp.int32)
    sds = jax.ShapeDtypeStruct

    rows, hidden = dense_gate.shape
    share = hidden // n_ep
    chips = n_ep // 2
    block = packed_rows(rows, share, seqs)
    groups = [[2 * chip + core for chip in range(chips)] for core in range(2)]
    swap = [(i, i ^ 1) for i in range(n_ep)]
    held = (
        tokens,
        norm1_gain[None],
        w_dt.T,
        dt_bias[None],
        a_log[None],
        d_skip[None],
        taps_x,
        taps_b,
        taps_c,
        group_gain[None],
        taps_first(conv_x),
        taps_first(conv_b),
        taps_first(conv_c),
        dense_gate,
        dense_up,
        dense_down.T,
        route_ids,
        route_weights,
        w_x,
        w_b,
        w_c,
        w_z,
        w_out,
        ssm_state,
    )
    part, scaled, keys, decay, kept, parted, conv_x_next, conv_b_next, conv_c_next = pl.pallas_call(
        functools.partial(mixer_kernel, n_tp=n_tp, held=len(held)),
        out_shape=(
            sds((seqs, model), bf16),
            sds((seqs, w_x.shape[1]), f32),
            sds((seqs, w_b.shape[1]), f32),
            sds((seqs, ssm_state.shape[1]), f32),
            sds((chips, block, LANES), bf16),
            sds((chips, block, LANES), bf16),
            *[sds(taps_first(value).shape, bf16) for value in (conv_x, conv_b, conv_c)],
        ),
        in_specs=[SMEM] + [HBM] * len(held),
        out_specs=(VMEM,) * 6 + (HBM,) * 3,
        scratch_shapes=[pltpu.VMEM(value.shape, value.dtype) for value in held]
        + [pltpu.VMEM(taps_first(value).shape, bf16) for value in (conv_x, conv_b, conv_c)]
        + [
            pltpu.SemaphoreType.DMA((len(held) - 1,)),
            pltpu.SemaphoreType.DMA((seqs,)),
            pltpu.SemaphoreType.DMA((3,)),
        ],
        compiler_params=pltpu.CompilerParams(vmem_limit_bytes=20 * MIB),
        name="mixer",
    )(place, *map(in_hbm, held))

    state_next = pl.pallas_call(
        advance_kernel,
        out_shape=sds(ssm_state.shape, f32),
        in_specs=[VMEM] * 3 + [HBM],
        out_specs=HBM,
        scratch_shapes=[
            pltpu.VMEM(ssm_state.shape, f32),
            pltpu.SemaphoreType.DMA((seqs,)),
            pltpu.SemaphoreType.DMA((seqs,)),
        ],
        compiler_params=pltpu.CompilerParams(vmem_limit_bytes=12 * MIB),
        name="advance",
    )(scaled, keys, decay, in_hbm(ssm_state))

    if n_tp == 2:
        other = lax.ppermute(part, "tp", [(0, 1), (1, 0)])
    else:
        gathered = lax.all_gather(part, "tp", axis=0).astype(f32)
        total = gathered[0]
        for i in range(1, n_tp):
            total = total + gathered[i]
        other = total - part.astype(f32)

    swapped = lax.ppermute(parted, "ep", swap)
    tile_rows = seqs * model // LANES
    spread, residual = pl.pallas_call(
        norm_kernel,
        out_shape=(sds((chips, tile_rows + 2 * block, LANES), bf16), sds((seqs, model), bf16)),
        in_specs=[VMEM] * 6,
        out_specs=(VMEM, VMEM),
        compiler_params=pltpu.CompilerParams(vmem_limit_bytes=4 * MIB),
        name="norm",
    )(tokens, part, other, norm2_gain[None], kept, swapped)
    got = lax.all_to_all(
        spread, "ep", split_axis=0, concat_axis=0, tiled=True, axis_index_groups=groups
    )
    got_other = lax.ppermute(got, "ep", swap)

    parts_shape = (chips * n_tp * seqs, model // n_tp)
    sizes = dict(share=share, seqs=seqs, n_tp=n_tp)
    expert_weights = (exp_gate, exp_up, exp_down, branch_gate)
    keep, wide, back, table = pl.pallas_call(
        functools.partial(own_experts_kernel, **sizes),
        out_shape=(
            sds(parts_shape, f32),
            sds((model, LANES), bf16),
            sds((model, LANES), bf16),
            sds((chips * seqs, LANES), f32),
        ),
        in_specs=[SMEM] + [VMEM] * 5,
        out_specs=(VMEM,) * 4,
        compiler_params=pltpu.CompilerParams(vmem_limit_bytes=12 * MIB),
        name="own_experts",
    )(place, got, *expert_weights)
    send = pl.pallas_call(
        functools.partial(other_experts_kernel, **sizes),
        out_shape=sds(parts_shape, bf16),
        in_specs=[VMEM] * 8,
        out_specs=VMEM,
        compiler_params=pltpu.CompilerParams(vmem_limit_bytes=12 * MIB),
        name="other_experts",
    )(got_other, *expert_weights, wide, back, table)
    outgoing = pl.pallas_call(
        add_kernel,
        out_shape=sds(parts_shape, bf16),
        in_specs=[VMEM] * 2,
        out_specs=VMEM,
        compiler_params=pltpu.CompilerParams(vmem_limit_bytes=4 * MIB),
        name="add",
    )(keep, lax.ppermute(send, "ep", swap))
    flat_groups = [[ep * n_tp + q for ep in group for q in range(n_tp)] for group in groups]
    parts = lax.all_to_all(
        outgoing,
        ("ep", "tp"),
        split_axis=0,
        concat_axis=0,
        tiled=True,
        axis_index_groups=flat_groups,
    )

    mixed = pl.pallas_call(
        functools.partial(sum_kernel, n_tp=n_tp),
        out_shape=sds((seqs, model // n_tp), bf16),
        in_specs=[SMEM, VMEM, VMEM],
        out_specs=VMEM,
        compiler_params=pltpu.CompilerParams(vmem_limit_bytes=4 * MIB),
        name="total",
    )(place, parts, residual)
    return (
        mixed,
        state_next,
        taps_first(conv_x_next),
        taps_first(conv_b_next),
        taps_first(conv_c_next),
    )


def solution(mesh):
    return jax.shard_map(
        body,
        mesh=mesh,
        in_specs=(
            P("ep", None),
            P("ep", "tp", None, None),
            P("ep", None, "tp"),
            P("ep", None, "tp"),
            P("ep", None, "tp"),
            P(None, "tp"),
            P(None, "tp"),
            P(None, "tp"),
            P(None, "tp"),
            P(),
            P("tp"),
            P("tp"),
            P("tp"),
            P(None, "tp"),
            P(None, "tp"),
            P(None, "tp"),
            P(),
            P("tp"),
            P("tp", None),
            P(),
            P("ep", None),
            P("ep", None),
            P("ep", None, "tp"),
            P("ep", None, "tp"),
            P("ep", "tp", None),
            P("ep", "tp"),
            P("ep", "tp"),
            P("tp", "ep"),
            P(),
        ),
        out_specs=(
            P("ep", "tp"),
            P("ep", "tp", None, None),
            P("ep", None, "tp"),
            P("ep", None, "tp"),
            P("ep", None, "tp"),
        ),
        check_vma=False,
    )
```

```python
import functools

import jax
import jax.numpy as jnp
from jax import lax
from jax.experimental import pallas as pl
from jax.experimental.pallas import tpu as pltpu
from jax.sharding import PartitionSpec as P


epsilon = 1e-06
f32 = jnp.float32
bf16 = jnp.bfloat16
VMEM = pl.BlockSpec(memory_space=pltpu.VMEM)
SMEM = pl.BlockSpec(memory_space=pltpu.SMEM)
HBM = pl.BlockSpec(memory_space=pltpu.HBM)
MIB = 1 << 20
LANES = 128


def dot(left, right):
    return lax.dot_general(left, right, (((1,), (0,)), ((), ())), preferred_element_type=f32)


def dot_nt(left, right):
    return lax.dot_general(left, right, (((1,), (1,)), ((), ())), preferred_element_type=f32)


def silu(value):
    return value / (1.0 + jnp.exp(-value))


def sigmoid(value):
    return 1.0 / (1.0 + jnp.exp(-value))


def rms_rows(values, gain):
    return values * lax.rsqrt(jnp.mean(values * values, axis=-1, keepdims=True) + epsilon) * gain


def spread_heads(values, width):
    rows, heads = values.shape
    return jnp.concatenate(
        [jnp.broadcast_to(values[:, h : h + 1], (rows, width)) for h in range(heads)], axis=1
    )


def in_hbm(values):
    return pltpu.with_memory_space_constraint(values, pltpu.HBM)


def taps_first(values):
    return values.transpose(1, 0, 2)


def fold_of(rows, share):
    fold = 1
    while 4 * fold * share <= LANES and rows % (32 * fold) == 0:
        fold *= 2
    return fold


def packed_rows(rows, share, seqs):
    fold = fold_of(rows, share)
    return rows // fold + rows // (2 * fold) + seqs


def side_by_side(values, fold):
    rows, width = values.shape
    count, stride = rows // fold, LANES // fold
    pieces = []
    for k in range(fold):
        pieces.append(values[k * count : (k + 1) * count])
        if stride > width:
            pieces.append(jnp.zeros((count, stride - width), f32))
    return jnp.concatenate(pieces, axis=1)


def pack(gate, up, down, ids, weights, chip, fold):
    seqs, _ = ids.shape
    tail = []
    for expert in (2 * chip, 2 * chip + 1):
        weight = jnp.sum(jnp.where(ids == expert, weights, 0.0), axis=1, keepdims=True)
        high = weight.astype(bf16).astype(f32)
        tail += [high, weight - high]
    tail = jnp.concatenate((*tail, jnp.zeros((seqs, LANES - 4), f32)), axis=1)
    both = side_by_side(jnp.concatenate((gate, up), axis=1), fold)
    return jnp.concatenate((both, side_by_side(down, 2 * fold), tail), axis=0)


def mixer_kernel(*refs, n_tp, held):
    tp_ref = refs[0]
    sources = refs[1 : 1 + held]
    part_ref, packed_ref = refs[1 + held : 3 + held]
    results = refs[3 + held : 9 + held]
    targets = refs[9 + held : 9 + 2 * held]
    buffers = refs[9 + 2 * held : 15 + 2 * held]
    scaled_ref, key_ref, decay_ref, conv_x_next, conv_b_next, conv_c_next = buffers
    in_sems, state_sems, out_sems = refs[15 + 2 * held :]
    (
        tokens_ref,
        gain_ref,
        w_dt_ref,
        dt_bias_ref,
        a_log_ref,
        d_skip_ref,
        taps_x_ref,
        taps_b_ref,
        taps_c_ref,
        group_gain_ref,
        conv_x_ref,
        conv_b_ref,
        conv_c_ref,
        gate_ref,
        up_ref,
        down_ref,
        ids_ref,
        weights_ref,
        w_x,
        w_b,
        w_c,
        w_z,
        w_out,
        state,
    ) = targets
    seqs, heads, head_dim, state_dim = state.shape
    channels = heads * head_dim
    groups = w_b.shape[1] // state_dim
    per_group = heads // groups
    width = channels // groups
    copy = pltpu.make_async_copy
    loads = [copy(sources[i], targets[i], in_sems.at[i]) for i in range(held - 1)]
    *small_loads, load_x, load_b, load_c, load_z, load_out = loads
    state_loads = [copy(sources[-1].at[s], state.at[s], state_sems.at[s]) for s in range(seqs)]
    stores = [copy(buffers[i], results[i], out_sems.at[i]) for i in range(6)]
    for load in [*small_loads, load_x, load_b, load_c, *state_loads, load_z, load_out]:
        load.start()
    for load in small_loads:
        load.wait()

    normed = rms_rows(tokens_ref[...].astype(f32), gain_ref[...]).astype(bf16)
    dt_all = dot_nt(normed, w_dt_ref[...])
    own = tp_ref[0]
    dt_raw = jnp.zeros((seqs, heads), f32)
    for i in range(n_tp):
        dt_raw += jnp.where(own == i, dt_all[:, i * heads : (i + 1) * heads], 0.0)
    shifted = dt_raw + dt_bias_ref[...]
    step = jnp.maximum(shifted, 0.0) + jnp.log1p(jnp.exp(-jnp.abs(shifted)))
    decay = jnp.exp(-step * jnp.exp(a_log_ref[...]))

    gate = gate_ref[...].astype(f32)
    up = up_ref[...].astype(f32)
    down = down_ref[...].astype(f32)
    ids = ids_ref[...]
    weights = weights_ref[...]
    chips = packed_ref.shape[0]
    share = gate.shape[1] // chips
    fold = fold_of(gate.shape[0], share)
    for chip in range(chips):
        part = slice(chip * share, (chip + 1) * share)
        packed_ref[chip] = pack(
            gate[:, part], up[:, part], down[:, part], ids, weights, chip, fold
        ).astype(bf16)

    def short_conv(previous_ref, fresh, taps_ref, out_ref):
        taps = taps_ref[...].astype(f32)
        last = taps.shape[0] - 1
        total = fresh * taps[last:]
        for k in range(last):
            total += previous_ref[k].astype(f32) * taps[k : k + 1]
            out_ref[k] = previous_ref[k + 1] if k + 1 < last else fresh.astype(bf16)
        return silu(total)

    def projected(ref):
        return dot(normed, ref[...]).astype(bf16).astype(f32)

    load_x.wait()
    xs = short_conv(conv_x_ref, projected(w_x), taps_x_ref, conv_x_next)
    load_b.wait()
    bs = short_conv(conv_b_ref, projected(w_b), taps_b_ref, conv_b_next)
    load_c.wait()
    cs = short_conv(conv_c_ref, projected(w_c), taps_c_ref, conv_c_next)
    queries = cs.astype(bf16)
    scaled = spread_heads(step, head_dim) * xs
    scaled_ref[...] = scaled
    key_ref[...] = bs
    decay_ref[...] = decay
    for store in stores:
        store.start()
    row = lax.broadcasted_iota(jnp.int32, (seqs, width), 0)
    readout = [jnp.zeros((seqs, width), f32) for _ in range(groups)]
    for s in range(seqs):
        state_loads[s].wait()
        for g in range(groups):
            block = state[s, g * per_group : (g + 1) * per_group].reshape(width, state_dim)
            read = dot_nt(queries[:, g * state_dim : (g + 1) * state_dim], block.astype(bf16))
            readout[g] = jnp.where(row == s, read, readout[g])
    load_z.wait()
    z_gate = silu(projected(w_z))
    skip = spread_heads(d_skip_ref[...], head_dim) * xs
    kept = spread_heads(decay, head_dim)
    mixed = []
    for g in range(groups):
        part = slice(g * width, (g + 1) * width)
        own = slice(g * state_dim, (g + 1) * state_dim)
        match = jnp.sum(bs[:, own] * cs[:, own], axis=1, keepdims=True)
        read = kept[:, part] * readout[g] + scaled[:, part] * match
        gated = (read + skip[:, part]) * z_gate[:, part]
        mixed.append(rms_rows(gated, group_gain_ref[:, part]).astype(bf16))
    load_out.wait()
    part_ref[...] = dot(jnp.concatenate(mixed, axis=1), w_out[...]).astype(bf16)
    for store in stores:
        store.wait()


def advance_kernel(
    scaled_hbm,
    key_hbm,
    decay_hbm,
    state_hbm,
    state_out,
    scaled_ref,
    key_ref,
    decay_ref,
    state,
    small_sems,
    in_sems,
    out_sems,
):
    seqs, heads, head_dim, state_dim = state.shape
    per_group = heads * state_dim // key_ref.shape[1]
    copy = pltpu.make_async_copy
    small_loads = [
        copy(scaled_hbm, scaled_ref, small_sems.at[0]),
        copy(key_hbm, key_ref, small_sems.at[1]),
        copy(decay_hbm, decay_ref, small_sems.at[2]),
    ]
    loads = [copy(state_hbm.at[s], state.at[s], in_sems.at[s]) for s in range(seqs)]
    stores = [copy(state.at[s], state_out.at[s], out_sems.at[s]) for s in range(seqs)]
    for load in [*small_loads, *loads]:
        load.start()
    for load in small_loads:
        load.wait()
    scaled = scaled_ref[...].T
    keys = key_ref[...]
    decay = decay_ref[...]
    for s in range(seqs):
        loads[s].wait()
        for h in range(heads):
            g = h // per_group
            key = keys[s : s + 1, g * state_dim : (g + 1) * state_dim]
            column = scaled[h * head_dim : (h + 1) * head_dim, s : s + 1]
            state[s, h] = decay[s : s + 1, h : h + 1] * state[s, h] + column * key
        stores[s].start()
    for store in stores:
        store.wait()


def norm_kernel(tokens_ref, own_ref, other_ref, gain_ref, packed_ref, spread_ref, residual_ref):
    _, model = tokens_ref.shape
    summed = own_ref[...].astype(f32) + other_ref[...].astype(f32)
    residual = (tokens_ref[...].astype(f32) + summed).astype(bf16)
    residual_ref[...] = residual
    normed = rms_rows(residual.astype(f32), gain_ref[...])
    tiles = jnp.concatenate(
        [normed[:, k * LANES : (k + 1) * LANES] for k in range(model // LANES)], axis=0
    ).astype(bf16)
    count = tiles.shape[0]
    for chip in range(packed_ref.shape[0]):
        spread_ref[chip, :count] = tiles
        spread_ref[chip, count:] = packed_ref[chip]


def token_rows(tiles_ref, seqs, model):
    rows = []
    for chip in range(tiles_ref.shape[0]):
        tiles = tiles_ref[chip, : seqs * model // LANES]
        rows.append(
            jnp.concatenate(
                [tiles[k * seqs : (k + 1) * seqs] for k in range(model // LANES)], axis=1
            )
        )
    return jnp.concatenate(rows, axis=0)


def experts_kernel(core_ref, got_ref, branch_ref, *refs, seqs, model):
    result_ref, rows_ref, scale_ref = refs[-3:]
    chips, total, _ = got_ref.shape
    core = core_ref[0]
    rows = token_rows(got_ref, seqs, model)
    table = jnp.concatenate(
        [got_ref[i, total - seqs :].astype(f32) for i in range(chips)], axis=0
    )
    lane = lax.broadcasted_iota(jnp.int32, table.shape, 1)
    result = jnp.zeros((chips * seqs, model), f32)
    for index in range(2):
        gate_ref, up_ref, down_ref = refs[3 * index : 3 * index + 3]
        expert = core if index == 0 else 1 - core
        weight = jnp.sum(jnp.where(lane // 2 == expert, table, 0.0), axis=1, keepdims=True)
        active = (silu(dot(rows, gate_ref[0])) * dot(rows, up_ref[0])).astype(bf16)
        result += weight * dot(active, down_ref[0])
    result_ref[...] = result
    rows_ref[...] = rows
    branch = sigmoid(
        jnp.sum(rows.astype(f32) * branch_ref[...].astype(f32)[None], axis=1, keepdims=True)
    )
    scale_ref[...] = jnp.broadcast_to(branch, scale_ref.shape)


def dense_kernel(
    core_ref, got_ref, other_ref, routed_ref, rows_ref, scale_ref, out_ref, wide_ref, back_ref, *, share, seqs, n_tp
):
    model = wide_ref.shape[0]
    chips = got_ref.shape[0]
    rows = model // (2 * chips)
    start = seqs * model // LANES
    fold = fold_of(rows, share)
    core = core_ref[0]
    wide_rows, back_rows = rows // fold, rows // (2 * fold)

    def unfold(values, count, target_ref, source):
        height = values.shape[0]
        target_ref[pl.ds(pl.multiple_of(source, 8), height)] = values
        wider = values.astype(f32)
        for k in range(1, count):
            moved = pltpu.roll(wider, LANES - k * LANES // count, 1).astype(bf16)
            target_ref[pl.ds(pl.multiple_of(source + k * height, 8), height)] = moved

    for chip in range(chips):
        for ref, parity in ((got_ref, core), (other_ref, 1 - core)):
            source = (2 * chip + parity) * rows
            wide = ref[chip, start : start + wide_rows]
            back = ref[chip, start + wide_rows : start + wide_rows + back_rows]
            unfold(wide, fold, wide_ref, source)
            unfold(back, 2 * fold, back_ref, source)
    own = rows_ref[...]
    hidden = dot(own, wide_ref[...])
    lane = lax.broadcasted_iota(jnp.int32, hidden.shape, 1)
    dense = silu(hidden) * pltpu.roll(hidden, LANES - share, 1)
    dense = jnp.where(lane < share, dense, 0.0).astype(bf16)
    result = routed_ref[...] + scale_ref[:, :1] * dot_nt(dense, back_ref[...])
    half = model // n_tp
    for i in range(chips):
        for q in range(n_tp):
            place = (i * n_tp + q) * seqs
            value = result[i * seqs : (i + 1) * seqs, q * half : (q + 1) * half]
            out_ref[place : place + seqs] = value.astype(bf16)


def sum_kernel(tp_ref, parts_ref, residual_ref, out_ref, *, n_tp):
    seqs, half = out_ref.shape
    own = tp_ref[0]
    total = jnp.zeros((seqs, half), f32)
    for q in range(n_tp):
        total += jnp.where(
            own == q, residual_ref[:, q * half : (q + 1) * half].astype(f32), 0.0
        )
    for i in range(parts_ref.shape[0] // seqs):
        total += parts_ref[i * seqs : (i + 1) * seqs].astype(f32)
    out_ref[...] = total.astype(bf16)


def body(
    tokens,
    ssm_state,
    conv_x,
    conv_b,
    conv_c,
    w_x,
    w_z,
    w_b,
    w_c,
    w_dt,
    dt_bias,
    a_log,
    d_skip,
    taps_x,
    taps_b,
    taps_c,
    norm1_gain,
    group_gain,
    w_out,
    norm2_gain,
    route_ids,
    route_weights,
    exp_gate,
    exp_up,
    exp_down,
    dense_gate,
    dense_up,
    dense_down,
    branch_gate,
):
    seqs, model = tokens.shape
    n_ep = lax.axis_size("ep")
    n_tp = lax.axis_size("tp")
    tp_index = lax.axis_index("tp").astype(jnp.int32)[None]
    core_index = (lax.axis_index("ep") % 2).astype(jnp.int32)[None]
    sds = jax.ShapeDtypeStruct

    rows, hidden = dense_gate.shape
    chips = n_ep // 2
    share = hidden // chips
    block = packed_rows(rows, share, seqs)
    groups = [[2 * chip + core for chip in range(chips)] for core in range(2)]
    swap = [(i, i ^ 1) for i in range(n_ep)]
    held = (
        tokens,
        norm1_gain[None],
        w_dt.T,
        dt_bias[None],
        a_log[None],
        d_skip[None],
        taps_x,
        taps_b,
        taps_c,
        group_gain[None],
        taps_first(conv_x),
        taps_first(conv_b),
        taps_first(conv_c),
        dense_gate,
        dense_up,
        dense_down.T,
        route_ids,
        route_weights,
        w_x,
        w_b,
        w_c,
        w_z,
        w_out,
        ssm_state,
    )
    results = (
        sds((seqs, w_x.shape[1]), f32),
        sds((seqs, w_b.shape[1]), f32),
        sds((seqs, ssm_state.shape[1]), f32),
        *[sds(taps_first(value).shape, bf16) for value in (conv_x, conv_b, conv_c)],
    )
    part, packed, scaled, keys, decay, conv_x_next, conv_b_next, conv_c_next = pl.pallas_call(
        functools.partial(mixer_kernel, n_tp=n_tp, held=len(held)),
        out_shape=(
            sds((seqs, model), bf16),
            sds((chips, block, LANES), bf16),
            *[pltpu.HBM(value.shape, value.dtype) for value in results],
        ),
        in_specs=[SMEM] + [HBM] * len(held),
        out_specs=(VMEM,) * 2 + (HBM,) * 6,
        scratch_shapes=[pltpu.VMEM(value.shape, value.dtype) for value in held]
        + [pltpu.VMEM(value.shape, value.dtype) for value in results]
        + [
            pltpu.SemaphoreType.DMA((len(held) - 1,)),
            pltpu.SemaphoreType.DMA((seqs,)),
            pltpu.SemaphoreType.DMA((len(results),)),
        ],
        compiler_params=pltpu.CompilerParams(vmem_limit_bytes=20 * MIB),
        name="mixer",
    )(tp_index, *map(in_hbm, held))

    state_next = pl.pallas_call(
        advance_kernel,
        out_shape=sds(ssm_state.shape, f32),
        in_specs=[HBM] * 4,
        out_specs=HBM,
        scratch_shapes=[
            *[pltpu.VMEM(value.shape, f32) for value in (scaled, keys, decay, ssm_state)],
            pltpu.SemaphoreType.DMA((3,)),
            pltpu.SemaphoreType.DMA((seqs,)),
            pltpu.SemaphoreType.DMA((seqs,)),
        ],
        compiler_params=pltpu.CompilerParams(vmem_limit_bytes=12 * MIB),
        name="advance",
    )(*map(in_hbm, (scaled, keys, decay, ssm_state)))

    if n_tp == 2:
        other = lax.ppermute(part, "tp", [(0, 1), (1, 0)])
    else:
        gathered = lax.all_gather(part, "tp", axis=0).astype(f32)
        total = gathered[0]
        for i in range(1, n_tp):
            total = total + gathered[i]
        other = total - part.astype(f32)

    tile_rows = seqs * model // LANES
    spread, residual = pl.pallas_call(
        norm_kernel,
        out_shape=(sds((chips, tile_rows + block, LANES), bf16), sds((seqs, model), bf16)),
        in_specs=[VMEM] * 5,
        out_specs=(VMEM, VMEM),
        compiler_params=pltpu.CompilerParams(vmem_limit_bytes=4 * MIB),
        name="norm",
    )(tokens, part, other, norm2_gain[None], packed)
    got = lax.all_to_all(
        spread, "ep", split_axis=0, concat_axis=0, tiled=True, axis_index_groups=groups
    )
    own_experts = (exp_gate, exp_up, exp_down)
    other_experts = [lax.ppermute(value, "ep", swap) for value in own_experts]
    got_other = lax.ppermute(got, "ep", swap)

    routed, own_rows, scale = pl.pallas_call(
        functools.partial(experts_kernel, seqs=seqs, model=model),
        out_shape=(
            sds((chips * seqs, model), f32),
            sds((chips * seqs, model), bf16),
            sds((chips * seqs, LANES), f32),
        ),
        in_specs=[SMEM] + [VMEM] * 8,
        out_specs=(VMEM,) * 3,
        compiler_params=pltpu.CompilerParams(vmem_limit_bytes=12 * MIB),
        name="experts",
    )(core_index, got, branch_gate, *own_experts, *other_experts)
    outgoing = pl.pallas_call(
        functools.partial(dense_kernel, share=share, seqs=seqs, n_tp=n_tp),
        out_shape=sds((chips * n_tp * seqs, model // n_tp), bf16),
        in_specs=[SMEM] + [VMEM] * 5,
        out_specs=VMEM,
        scratch_shapes=[pltpu.VMEM((model, LANES), bf16), pltpu.VMEM((model, LANES), bf16)],
        compiler_params=pltpu.CompilerParams(vmem_limit_bytes=8 * MIB),
        name="dense",
    )(core_index, got, got_other, routed, own_rows, scale)
    flat_groups = [[ep * n_tp + q for ep in group for q in range(n_tp)] for group in groups]
    parts = lax.all_to_all(
        outgoing,
        ("ep", "tp"),
        split_axis=0,
        concat_axis=0,
        tiled=True,
        axis_index_groups=flat_groups,
    )

    mixed = pl.pallas_call(
        functools.partial(sum_kernel, n_tp=n_tp),
        out_shape=sds((seqs, model // n_tp), bf16),
        in_specs=[SMEM, VMEM, VMEM],
        out_specs=VMEM,
        compiler_params=pltpu.CompilerParams(vmem_limit_bytes=4 * MIB),
        name="total",
    )(tp_index, parts, residual)
    return (
        mixed,
        state_next,
        taps_first(conv_x_next),
        taps_first(conv_b_next),
        taps_first(conv_c_next),
    )


def solution(mesh):
    return jax.shard_map(
        body,
        mesh=mesh,
        in_specs=(
            P("ep", None),
            P("ep", "tp", None, None),
            P("ep", None, "tp"),
            P("ep", None, "tp"),
            P("ep", None, "tp"),
            P(None, "tp"),
            P(None, "tp"),
            P(None, "tp"),
            P(None, "tp"),
            P(),
            P("tp"),
            P("tp"),
            P("tp"),
            P(None, "tp"),
            P(None, "tp"),
            P(None, "tp"),
            P(),
            P("tp"),
            P("tp", None),
            P(),
            P("ep", None),
            P("ep", None),
            P("ep", None, "tp"),
            P("ep", None, "tp"),
            P("ep", "tp", None),
            P("ep", "tp"),
            P("ep", "tp"),
            P("tp", "ep"),
            P(),
        ),
        out_specs=(
            P("ep", "tp"),
            P("ep", "tp", None, None),
            P("ep", None, "tp"),
            P("ep", None, "tp"),
            P("ep", None, "tp"),
        ),
        check_vma=False,
    )
```

```python
import functools

import jax
import jax.numpy as jnp
from jax import lax
from jax.experimental import pallas as pl
from jax.experimental.pallas import tpu as pltpu
from jax.sharding import PartitionSpec as P


epsilon = 1e-06
f32 = jnp.float32
bf16 = jnp.bfloat16
VMEM = pl.BlockSpec(memory_space=pltpu.VMEM)
SMEM = pl.BlockSpec(memory_space=pltpu.SMEM)
HBM = pl.BlockSpec(memory_space=pltpu.HBM)
MIB = 1 << 20
LANES = 128


def dot(left, right):
    return lax.dot_general(left, right, (((1,), (0,)), ((), ())), preferred_element_type=f32)


def dot_nt(left, right):
    return lax.dot_general(left, right, (((1,), (1,)), ((), ())), preferred_element_type=f32)


def silu(value):
    return value / (1.0 + jnp.exp(-value))


def sigmoid(value):
    return 1.0 / (1.0 + jnp.exp(-value))


def rms_rows(values, gain):
    return values * lax.rsqrt(jnp.mean(values * values, axis=-1, keepdims=True) + epsilon) * gain


def spread_heads(values, width):
    rows, heads = values.shape
    return jnp.concatenate(
        [jnp.broadcast_to(values[:, h : h + 1], (rows, width)) for h in range(heads)], axis=1
    )


def in_hbm(values):
    return pltpu.with_memory_space_constraint(values, pltpu.HBM)


def taps_first(values):
    return values.transpose(1, 0, 2)


def fold_of(rows, share):
    fold = 1
    while 4 * fold * share <= LANES and rows % (32 * fold) == 0:
        fold *= 2
    return fold


def back_fold_of(rows, share):
    fold = 1
    while 2 * fold * rows <= LANES and share % (16 * fold) == 0:
        fold *= 2
    return fold


def packed_rows(rows, share, seqs):
    return rows // fold_of(rows, share) + share // back_fold_of(rows, share) + seqs


def side_by_side(values, fold):
    rows, width = values.shape
    count, stride = rows // fold, LANES // fold
    pieces = []
    for k in range(fold):
        pieces.append(values[k * count : (k + 1) * count])
        if stride > width:
            pieces.append(jnp.zeros((count, stride - width), f32))
    return jnp.concatenate(pieces, axis=1)


def pack(gate, up, down, ids, weights, chip):
    seqs, _ = ids.shape
    tail = []
    for expert in (2 * chip, 2 * chip + 1):
        weight = jnp.sum(jnp.where(ids == expert, weights, 0.0), axis=1, keepdims=True)
        high = weight.astype(bf16).astype(f32)
        tail += [high, weight - high]
    tail = jnp.concatenate((*tail, jnp.zeros((seqs, LANES - 4), f32)), axis=1)
    rows, share = gate.shape
    both = side_by_side(jnp.concatenate((gate, up), axis=1), fold_of(rows, share))
    back = side_by_side(down, back_fold_of(rows, share))
    return jnp.concatenate((both, back, tail), axis=0)


def mixer_kernel(*refs, n_tp, held):
    tp_ref = refs[0]
    sources = refs[1 : 1 + held]
    part_ref, packed_ref = refs[1 + held : 3 + held]
    results = refs[3 + held : 9 + held]
    targets = refs[9 + held : 9 + 2 * held]
    buffers = refs[9 + 2 * held : 15 + 2 * held]
    scaled_ref, key_ref, decay_ref, conv_x_next, conv_b_next, conv_c_next = buffers
    in_sems, state_sems, out_sems = refs[15 + 2 * held :]
    (
        tokens_ref,
        gain_ref,
        w_dt_ref,
        dt_bias_ref,
        a_log_ref,
        d_skip_ref,
        taps_x_ref,
        taps_b_ref,
        taps_c_ref,
        group_gain_ref,
        conv_x_ref,
        conv_b_ref,
        conv_c_ref,
        gate_ref,
        up_ref,
        down_ref,
        ids_ref,
        weights_ref,
        w_x,
        w_b,
        w_c,
        w_z,
        w_out,
        state,
    ) = targets
    seqs, heads, head_dim, state_dim = state.shape
    channels = heads * head_dim
    groups = w_b.shape[1] // state_dim
    per_group = heads // groups
    width = channels // groups
    copy = pltpu.make_async_copy
    loads = [copy(sources[i], targets[i], in_sems.at[i]) for i in range(held - 1)]
    *small_loads, load_x, load_b, load_c, load_z, load_out = loads
    batch = seqs // 2
    state_loads = [
        copy(
            sources[-1].at[pl.ds(i * batch, batch)],
            state.at[pl.ds(i * batch, batch)],
            state_sems.at[i],
        )
        for i in range(2)
    ]
    stores = [copy(buffers[i], results[i], out_sems.at[i]) for i in range(6)]
    for load in [*small_loads, load_x, load_b, load_c, *state_loads, load_z, load_out]:
        load.start()
    for load in small_loads:
        load.wait()

    normed = rms_rows(tokens_ref[...].astype(f32), gain_ref[...]).astype(bf16)
    dt_all = dot_nt(normed, w_dt_ref[...])
    own = tp_ref[0]
    dt_raw = jnp.zeros((seqs, heads), f32)
    for i in range(n_tp):
        dt_raw += jnp.where(own == i, dt_all[:, i * heads : (i + 1) * heads], 0.0)
    shifted = dt_raw + dt_bias_ref[...]
    step = jnp.maximum(shifted, 0.0) + jnp.log1p(jnp.exp(-jnp.abs(shifted)))
    decay = jnp.exp(-step * jnp.exp(a_log_ref[...]))

    gate = gate_ref[...].astype(f32)
    up = up_ref[...].astype(f32)
    down = down_ref[...].astype(f32).T
    ids = ids_ref[...]
    weights = weights_ref[...]
    chips = packed_ref.shape[0]
    share = gate.shape[1] // chips
    for chip in range(chips):
        part = slice(chip * share, (chip + 1) * share)
        packed_ref[chip] = pack(
            gate[:, part], up[:, part], down[part], ids, weights, chip
        ).astype(bf16)

    def short_conv(previous_ref, fresh, taps_ref, out_ref):
        taps = taps_ref[...].astype(f32)
        last = taps.shape[0] - 1
        total = fresh * taps[last:]
        for k in range(last):
            total += previous_ref[k].astype(f32) * taps[k : k + 1]
            out_ref[k] = previous_ref[k + 1] if k + 1 < last else fresh.astype(bf16)
        return silu(total)

    def projected(ref):
        return dot(normed, ref[...]).astype(bf16).astype(f32)

    load_x.wait()
    xs = short_conv(conv_x_ref, projected(w_x), taps_x_ref, conv_x_next)
    load_b.wait()
    bs = short_conv(conv_b_ref, projected(w_b), taps_b_ref, conv_b_next)
    load_c.wait()
    cs = short_conv(conv_c_ref, projected(w_c), taps_c_ref, conv_c_next)
    queries = cs.astype(bf16)
    scaled = spread_heads(step, head_dim) * xs
    scaled_ref[...] = scaled
    key_ref[...] = bs
    decay_ref[...] = decay
    for store in stores:
        store.start()
    row = lax.broadcasted_iota(jnp.int32, (seqs, width), 0)
    readout = [jnp.zeros((seqs, width), f32) for _ in range(groups)]
    for s in range(seqs):
        if s % batch == 0:
            state_loads[s // batch].wait()
        for g in range(groups):
            block = state[s, g * per_group : (g + 1) * per_group].reshape(width, state_dim)
            read = dot_nt(queries[:, g * state_dim : (g + 1) * state_dim], block.astype(bf16))
            readout[g] = jnp.where(row == s, read, readout[g])
    load_z.wait()
    z_gate = silu(projected(w_z))
    skip = spread_heads(d_skip_ref[...], head_dim) * xs
    kept = spread_heads(decay, head_dim)
    mixed = []
    for g in range(groups):
        part = slice(g * width, (g + 1) * width)
        own = slice(g * state_dim, (g + 1) * state_dim)
        match = jnp.sum(bs[:, own] * cs[:, own], axis=1, keepdims=True)
        read = kept[:, part] * readout[g] + scaled[:, part] * match
        gated = (read + skip[:, part]) * z_gate[:, part]
        mixed.append(rms_rows(gated, group_gain_ref[:, part]).astype(bf16))
    load_out.wait()
    part_ref[...] = dot(jnp.concatenate(mixed, axis=1), w_out[...]).astype(bf16)
    for store in stores:
        store.wait()


def advance_kernel(
    scaled_hbm,
    key_hbm,
    decay_hbm,
    state_hbm,
    state_out,
    scaled_ref,
    key_ref,
    decay_ref,
    state,
    small_sems,
    in_sems,
    out_sems,
):
    seqs, heads, head_dim, state_dim = state.shape
    per_group = heads * state_dim // key_ref.shape[1]
    copy = pltpu.make_async_copy
    small_loads = [
        copy(scaled_hbm, scaled_ref, small_sems.at[0]),
        copy(key_hbm, key_ref, small_sems.at[1]),
        copy(decay_hbm, decay_ref, small_sems.at[2]),
    ]
    batch = max(1, seqs // 4)
    spans = [pl.ds(first, batch) for first in range(0, seqs, batch)]
    loads = [copy(state_hbm.at[p], state.at[p], in_sems.at[i]) for i, p in enumerate(spans)]
    stores = [copy(state.at[p], state_out.at[p], out_sems.at[i]) for i, p in enumerate(spans)]
    for load in [*small_loads, *loads]:
        load.start()
    for load in small_loads:
        load.wait()
    scaled = scaled_ref[...].T
    keys = key_ref[...]
    decay = decay_ref[...]
    for s in range(seqs):
        if s % batch == 0:
            loads[s // batch].wait()
        for h in range(heads):
            g = h // per_group
            key = keys[s : s + 1, g * state_dim : (g + 1) * state_dim]
            column = scaled[h * head_dim : (h + 1) * head_dim, s : s + 1]
            state[s, h] = decay[s : s + 1, h : h + 1] * state[s, h] + column * key
        if (s + 1) % batch == 0:
            stores[s // batch].start()
    for store in stores:
        store.wait()


def norm_kernel(tokens_ref, own_ref, other_ref, gain_ref, packed_ref, spread_ref, residual_ref):
    _, model = tokens_ref.shape
    summed = own_ref[...].astype(f32) + other_ref[...].astype(f32)
    residual = (tokens_ref[...].astype(f32) + summed).astype(bf16)
    residual_ref[...] = residual
    normed = rms_rows(residual.astype(f32), gain_ref[...])
    tiles = jnp.concatenate(
        [normed[:, k * LANES : (k + 1) * LANES] for k in range(model // LANES)], axis=0
    ).astype(bf16)
    count = tiles.shape[0]
    for chip in range(packed_ref.shape[0]):
        spread_ref[chip, :count] = tiles
        spread_ref[chip, count:] = packed_ref[chip]


def token_rows(tiles_ref, seqs, model):
    rows = []
    for chip in range(tiles_ref.shape[0]):
        tiles = tiles_ref[chip, : seqs * model // LANES]
        rows.append(
            jnp.concatenate(
                [tiles[k * seqs : (k + 1) * seqs] for k in range(model // LANES)], axis=1
            )
        )
    return jnp.concatenate(rows, axis=0)


def unfold(packed_ref, parity, start, share, wide_ref):
    chips = packed_ref.shape[0]
    rows = wide_ref.shape[0] // (2 * chips)
    fold = fold_of(rows, share)
    height = rows // fold
    wide_ref[...] = jnp.zeros(wide_ref.shape, bf16)
    for chip in range(chips):
        source = (2 * chip + parity) * rows
        values = packed_ref[chip, start : start + height]
        wide_ref[pl.ds(pl.multiple_of(source, 8), height)] = values
        wider = values.astype(f32)
        for k in range(1, fold):
            moved = pltpu.roll(wider, LANES - k * LANES // fold, 1).astype(bf16)
            wide_ref[pl.ds(pl.multiple_of(source + k * height, 8), height)] = moved


def down_rows(own_ref, other_ref, first, start, share, rows):
    fold = back_fold_of(rows, share)
    height, stride = share // fold, LANES // fold
    pieces = []
    for chip in range(own_ref.shape[0]):
        own, other = [
            jnp.concatenate(
                [values[:, k * stride : k * stride + rows] for k in range(fold)], axis=0
            )
            for values in (
                own_ref[chip, start : start + height].astype(f32),
                other_ref[chip, start : start + height].astype(f32),
            )
        ]
        pieces += [jnp.where(first, own, other), jnp.where(first, other, own)]
    return jnp.concatenate(pieces, axis=1).astype(bf16)


def experts_kernel(core_ref, got_ref, branch_ref, *refs, share, seqs, model):
    gate, up, other_gate, other_up, other_down, down_hbm = refs[:6]
    result_ref, rows_ref, hidden_ref, scale_ref, wide_ref, down, sem = refs[6:]
    load = pltpu.make_async_copy(down_hbm, down, sem.at[0])
    load.start()
    chips, total, _ = got_ref.shape
    core = core_ref[0]
    rows = token_rows(got_ref, seqs, model)
    rows_ref[...] = rows
    table = jnp.concatenate(
        [got_ref[i, total - seqs :].astype(f32) for i in range(chips)], axis=0
    )
    lane = lax.broadcasted_iota(jnp.int32, table.shape, 1)

    def active(gate_ref, up_ref):
        return (silu(dot(rows, gate_ref[0])) * dot(rows, up_ref[0])).astype(bf16)

    def weight_of(expert):
        return jnp.sum(jnp.where(lane // 2 == expert, table, 0.0), axis=1, keepdims=True)

    own_active = active(gate, up)
    other = weight_of(1 - core) * dot(active(other_gate, other_up), other_down[0])
    branch = sigmoid(
        jnp.sum(rows.astype(f32) * branch_ref[...].astype(f32)[None], axis=1, keepdims=True)
    )
    scale_ref[...] = jnp.broadcast_to(branch, scale_ref.shape)
    unfold(got_ref, core, seqs * model // LANES, share, wide_ref)
    hidden_ref[...] = dot(rows, wide_ref[...])
    load.wait()
    result_ref[...] = other + weight_of(core) * dot(own_active, down[0])


def dense_kernel(
    core_ref,
    own_ref,
    other_ref,
    routed_ref,
    rows_ref,
    half_ref,
    scale_ref,
    out_ref,
    wide_ref,
    *,
    share,
    seqs,
    n_tp,
):
    model = wide_ref.shape[0]
    chips = other_ref.shape[0]
    rows = model // (2 * chips)
    core = core_ref[0]
    start = seqs * model // LANES
    unfold(other_ref, 1 - core, start, share, wide_ref)
    hidden = half_ref[...] + dot(rows_ref[...], wide_ref[...])
    dense = silu(hidden) * pltpu.roll(hidden, LANES - share, 1)
    start += rows // fold_of(rows, share)
    back = down_rows(own_ref, other_ref, core == 0, start, share, rows)
    dense_out = dot(dense[:, :share].astype(bf16), back)
    result = routed_ref[...] + scale_ref[:, :1] * dense_out
    half = model // n_tp
    for i in range(chips):
        for q in range(n_tp):
            place = (i * n_tp + q) * seqs
            value = result[i * seqs : (i + 1) * seqs, q * half : (q + 1) * half]
            out_ref[place : place + seqs] = value.astype(bf16)


def sum_kernel(tp_ref, parts_ref, residual_ref, out_ref, *, n_tp):
    seqs, half = out_ref.shape
    own = tp_ref[0]
    total = jnp.zeros((seqs, half), f32)
    for q in range(n_tp):
        total += jnp.where(
            own == q, residual_ref[:, q * half : (q + 1) * half].astype(f32), 0.0
        )
    for i in range(parts_ref.shape[0] // seqs):
        total += parts_ref[i * seqs : (i + 1) * seqs].astype(f32)
    out_ref[...] = total.astype(bf16)


def body(
    tokens,
    ssm_state,
    conv_x,
    conv_b,
    conv_c,
    w_x,
    w_z,
    w_b,
    w_c,
    w_dt,
    dt_bias,
    a_log,
    d_skip,
    taps_x,
    taps_b,
    taps_c,
    norm1_gain,
    group_gain,
    w_out,
    norm2_gain,
    route_ids,
    route_weights,
    exp_gate,
    exp_up,
    exp_down,
    dense_gate,
    dense_up,
    dense_down,
    branch_gate,
):
    seqs, model = tokens.shape
    n_ep = lax.axis_size("ep")
    n_tp = lax.axis_size("tp")
    tp_index = lax.axis_index("tp").astype(jnp.int32)[None]
    core_index = (lax.axis_index("ep") % 2).astype(jnp.int32)[None]
    sds = jax.ShapeDtypeStruct

    rows, hidden = dense_gate.shape
    chips = n_ep // 2
    share = hidden // chips
    block = packed_rows(rows, share, seqs)
    groups = [[2 * chip + core for chip in range(chips)] for core in range(2)]
    swap = [(i, i ^ 1) for i in range(n_ep)]
    held = (
        tokens,
        norm1_gain[None],
        w_dt.T,
        dt_bias[None],
        a_log[None],
        d_skip[None],
        taps_x,
        taps_b,
        taps_c,
        group_gain[None],
        taps_first(conv_x),
        taps_first(conv_b),
        taps_first(conv_c),
        dense_gate,
        dense_up,
        dense_down.T,
        route_ids,
        route_weights,
        w_x,
        w_b,
        w_c,
        w_z,
        w_out,
        ssm_state,
    )
    results = (
        sds((seqs, w_x.shape[1]), f32),
        sds((seqs, w_b.shape[1]), f32),
        sds((seqs, ssm_state.shape[1]), f32),
        *[sds(taps_first(value).shape, bf16) for value in (conv_x, conv_b, conv_c)],
    )
    part, packed, scaled, keys, decay, conv_x_next, conv_b_next, conv_c_next = pl.pallas_call(
        functools.partial(mixer_kernel, n_tp=n_tp, held=len(held)),
        out_shape=(
            sds((seqs, model), bf16),
            sds((chips, block, LANES), bf16),
            *[pltpu.HBM(value.shape, value.dtype) for value in results],
        ),
        in_specs=[SMEM] + [HBM] * len(held),
        out_specs=(VMEM,) * 2 + (HBM,) * 6,
        scratch_shapes=[pltpu.VMEM(value.shape, value.dtype) for value in held]
        + [pltpu.VMEM(value.shape, value.dtype) for value in results]
        + [
            pltpu.SemaphoreType.DMA((len(held) - 1,)),
            pltpu.SemaphoreType.DMA((seqs,)),
            pltpu.SemaphoreType.DMA((len(results),)),
        ],
        compiler_params=pltpu.CompilerParams(vmem_limit_bytes=20 * MIB),
        name="mixer",
    )(tp_index, *map(in_hbm, held))

    state_next = pl.pallas_call(
        advance_kernel,
        out_shape=sds(ssm_state.shape, f32),
        in_specs=[HBM] * 4,
        out_specs=HBM,
        scratch_shapes=[
            *[pltpu.VMEM(value.shape, f32) for value in (scaled, keys, decay, ssm_state)],
            pltpu.SemaphoreType.DMA((3,)),
            pltpu.SemaphoreType.DMA((seqs,)),
            pltpu.SemaphoreType.DMA((seqs,)),
        ],
        compiler_params=pltpu.CompilerParams(vmem_limit_bytes=12 * MIB),
        name="advance",
    )(*map(in_hbm, (scaled, keys, decay, ssm_state)))

    if n_tp == 2:
        other = lax.ppermute(part, "tp", [(0, 1), (1, 0)])
    else:
        gathered = lax.all_gather(part, "tp", axis=0).astype(f32)
        total = gathered[0]
        for i in range(1, n_tp):
            total = total + gathered[i]
        other = total - part.astype(f32)

    tile_rows = seqs * model // LANES
    spread, residual = pl.pallas_call(
        norm_kernel,
        out_shape=(sds((chips, tile_rows + block, LANES), bf16), sds((seqs, model), bf16)),
        in_specs=[VMEM] * 5,
        out_specs=(VMEM, VMEM),
        compiler_params=pltpu.CompilerParams(vmem_limit_bytes=4 * MIB),
        name="norm",
    )(tokens, part, other, norm2_gain[None], packed)
    got = lax.all_to_all(
        spread, "ep", split_axis=0, concat_axis=0, tiled=True, axis_index_groups=groups
    )
    own_experts = (exp_gate, exp_up, exp_down)
    other_experts = [lax.ppermute(value, "ep", swap) for value in own_experts]
    got_other = lax.ppermute(got, "ep", swap)

    dense_inputs = pl.pallas_call(
        functools.partial(experts_kernel, share=share, seqs=seqs, model=model),
        out_shape=(
            sds((chips * seqs, model), f32),
            sds((chips * seqs, model), bf16),
            sds((chips * seqs, LANES), f32),
            sds((chips * seqs, LANES), f32),
        ),
        in_specs=[SMEM] + [VMEM] * 7 + [HBM],
        out_specs=(VMEM,) * 4,
        scratch_shapes=[
            pltpu.VMEM((model, LANES), bf16),
            pltpu.VMEM(exp_down.shape, bf16),
            pltpu.SemaphoreType.DMA((1,)),
        ],
        compiler_params=pltpu.CompilerParams(vmem_limit_bytes=12 * MIB),
        name="experts",
    )(core_index, got, branch_gate, exp_gate, exp_up, *other_experts, in_hbm(exp_down))
    outgoing = pl.pallas_call(
        functools.partial(dense_kernel, share=share, seqs=seqs, n_tp=n_tp),
        out_shape=sds((chips * n_tp * seqs, model // n_tp), bf16),
        in_specs=[SMEM] + [VMEM] * 6,
        out_specs=VMEM,
        scratch_shapes=[pltpu.VMEM((model, LANES), bf16)],
        compiler_params=pltpu.CompilerParams(vmem_limit_bytes=8 * MIB),
        name="dense",
    )(core_index, got, got_other, *dense_inputs)
    flat_groups = [[ep * n_tp + q for ep in group for q in range(n_tp)] for group in groups]
    parts = lax.all_to_all(
        outgoing,
        ("ep", "tp"),
        split_axis=0,
        concat_axis=0,
        tiled=True,
        axis_index_groups=flat_groups,
    )

    mixed = pl.pallas_call(
        functools.partial(sum_kernel, n_tp=n_tp),
        out_shape=sds((seqs, model // n_tp), bf16),
        in_specs=[SMEM, VMEM, VMEM],
        out_specs=VMEM,
        compiler_params=pltpu.CompilerParams(vmem_limit_bytes=4 * MIB),
        name="total",
    )(tp_index, parts, residual)
    return (
        mixed,
        state_next,
        taps_first(conv_x_next),
        taps_first(conv_b_next),
        taps_first(conv_c_next),
    )


def solution(mesh):
    return jax.shard_map(
        body,
        mesh=mesh,
        in_specs=(
            P("ep", None),
            P("ep", "tp", None, None),
            P("ep", None, "tp"),
            P("ep", None, "tp"),
            P("ep", None, "tp"),
            P(None, "tp"),
            P(None, "tp"),
            P(None, "tp"),
            P(None, "tp"),
            P(),
            P("tp"),
            P("tp"),
            P("tp"),
            P(None, "tp"),
            P(None, "tp"),
            P(None, "tp"),
            P(),
            P("tp"),
            P("tp", None),
            P(),
            P("ep", None),
            P("ep", None),
            P("ep", None, "tp"),
            P("ep", None, "tp"),
            P("ep", "tp", None),
            P("ep", "tp"),
            P("ep", "tp"),
            P("tp", "ep"),
            P(),
        ),
        out_specs=(
            P("ep", "tp"),
            P("ep", "tp", None, None),
            P("ep", None, "tp"),
            P("ep", None, "tp"),
            P("ep", None, "tp"),
        ),
        check_vma=False,
    )
```

```python
import functools

import jax
import jax.numpy as jnp
from jax import lax
from jax.experimental import pallas as pl
from jax.experimental.pallas import tpu as pltpu
from jax.sharding import PartitionSpec as P


epsilon = 1e-06
f32 = jnp.float32
bf16 = jnp.bfloat16
VMEM = pl.BlockSpec(memory_space=pltpu.VMEM)
SMEM = pl.BlockSpec(memory_space=pltpu.SMEM)
HBM = pl.BlockSpec(memory_space=pltpu.HBM)
MIB = 1 << 20
LANES = 128


def dot(left, right):
    return lax.dot_general(left, right, (((1,), (0,)), ((), ())), preferred_element_type=f32)


def dot_nt(left, right):
    return lax.dot_general(left, right, (((1,), (1,)), ((), ())), preferred_element_type=f32)


def silu(value):
    return value / (1.0 + jnp.exp(-value))


def sigmoid(value):
    return 1.0 / (1.0 + jnp.exp(-value))


def rms_rows(values, gain):
    return values * lax.rsqrt(jnp.mean(values * values, axis=-1, keepdims=True) + epsilon) * gain


def spread_heads(values, width):
    rows, heads = values.shape
    return jnp.concatenate(
        [jnp.broadcast_to(values[:, h : h + 1], (rows, width)) for h in range(heads)], axis=1
    )


def in_hbm(values):
    return pltpu.with_memory_space_constraint(values, pltpu.HBM)


def taps_first(values):
    return values.transpose(1, 0, 2)


def fold_of(rows, share):
    fold = 1
    while 4 * fold * share <= LANES and rows % (32 * fold) == 0:
        fold *= 2
    return fold


def back_fold_of(rows, share):
    fold = 1
    while 2 * fold * rows <= LANES and share % (16 * fold) == 0:
        fold *= 2
    return fold


def packed_rows(rows, share, seqs):
    return rows // fold_of(rows, share) + share // back_fold_of(rows, share) + seqs


def side_by_side(values, fold):
    rows, width = values.shape
    count, stride = rows // fold, LANES // fold
    pieces = []
    for k in range(fold):
        pieces.append(values[k * count : (k + 1) * count])
        if stride > width:
            pieces.append(jnp.zeros((count, stride - width), f32))
    return jnp.concatenate(pieces, axis=1)


def pack(gate, up, down, ids, weights, chip):
    seqs, _ = ids.shape
    tail = []
    for expert in (2 * chip, 2 * chip + 1):
        weight = jnp.sum(jnp.where(ids == expert, weights, 0.0), axis=1, keepdims=True)
        high = weight.astype(bf16).astype(f32)
        tail += [high, weight - high]
    tail = jnp.concatenate((*tail, jnp.zeros((seqs, LANES - 4), f32)), axis=1)
    rows, share = gate.shape
    both = side_by_side(jnp.concatenate((gate, up), axis=1), fold_of(rows, share))
    back = side_by_side(down, back_fold_of(rows, share))
    return jnp.concatenate((both, back, tail), axis=0)


def mixer_kernel(*refs, n_tp, held):
    tp_ref = refs[0]
    sources = refs[1 : 1 + held]
    part_ref, packed_ref = refs[1 + held : 3 + held]
    results = refs[3 + held : 9 + held]
    targets = refs[9 + held : 9 + 2 * held]
    buffers = refs[9 + 2 * held : 15 + 2 * held]
    scaled_ref, key_ref, decay_ref, conv_x_next, conv_b_next, conv_c_next = buffers
    in_sems, state_sems, out_sems = refs[15 + 2 * held :]
    (
        tokens_ref,
        gain_ref,
        w_dt_ref,
        dt_bias_ref,
        a_log_ref,
        d_skip_ref,
        taps_x_ref,
        taps_b_ref,
        taps_c_ref,
        group_gain_ref,
        conv_x_ref,
        conv_b_ref,
        conv_c_ref,
        gate_ref,
        up_ref,
        down_ref,
        ids_ref,
        weights_ref,
        w_x,
        w_b,
        w_c,
        w_z,
        w_out,
        state,
    ) = targets
    seqs, heads, head_dim, state_dim = state.shape
    channels = heads * head_dim
    groups = w_b.shape[1] // state_dim
    per_group = heads // groups
    width = channels // groups
    copy = pltpu.make_async_copy
    loads = [copy(sources[i], targets[i], in_sems.at[i]) for i in range(held - 1)]
    *small_loads, load_x, load_b, load_c, load_z, load_out = loads
    batch = seqs // 2
    state_loads = [
        copy(
            sources[-1].at[pl.ds(i * batch, batch)],
            state.at[pl.ds(i * batch, batch)],
            state_sems.at[i],
        )
        for i in range(2)
    ]
    stores = [copy(buffers[i], results[i], out_sems.at[i]) for i in range(6)]
    for load in [*small_loads[:2], load_x, *small_loads[2:], load_b, load_c, *state_loads, load_z, load_out]:
        load.start()
    for load in small_loads:
        load.wait()

    normed = rms_rows(tokens_ref[...].astype(f32), gain_ref[...]).astype(bf16)
    dt_all = dot_nt(normed, w_dt_ref[...])
    own = tp_ref[0]
    dt_raw = jnp.zeros((seqs, heads), f32)
    for i in range(n_tp):
        dt_raw += jnp.where(own == i, dt_all[:, i * heads : (i + 1) * heads], 0.0)
    shifted = dt_raw + dt_bias_ref[...]
    step = jnp.maximum(shifted, 0.0) + jnp.log1p(jnp.exp(-jnp.abs(shifted)))
    decay = jnp.exp(-step * jnp.exp(a_log_ref[...]))

    gate = gate_ref[...].astype(f32)
    up = up_ref[...].astype(f32)
    down = down_ref[...].astype(f32).T
    ids = ids_ref[...]
    weights = weights_ref[...]
    chips = packed_ref.shape[0]
    share = gate.shape[1] // chips
    for chip in range(chips):
        part = slice(chip * share, (chip + 1) * share)
        packed_ref[chip] = pack(
            gate[:, part], up[:, part], down[part], ids, weights, chip
        ).astype(bf16)

    def short_conv(previous_ref, fresh, taps_ref, out_ref):
        taps = taps_ref[...].astype(f32)
        last = taps.shape[0] - 1
        total = fresh * taps[last:]
        for k in range(last):
            total += previous_ref[k].astype(f32) * taps[k : k + 1]
            out_ref[k] = previous_ref[k + 1] if k + 1 < last else fresh.astype(bf16)
        return silu(total)

    def projected(ref):
        return dot(normed, ref[...]).astype(bf16).astype(f32)

    load_x.wait()
    xs = short_conv(conv_x_ref, projected(w_x), taps_x_ref, conv_x_next)
    load_b.wait()
    bs = short_conv(conv_b_ref, projected(w_b), taps_b_ref, conv_b_next)
    load_c.wait()
    cs = short_conv(conv_c_ref, projected(w_c), taps_c_ref, conv_c_next)
    queries = cs.astype(bf16)
    scaled = spread_heads(step, head_dim) * xs
    scaled_ref[...] = scaled
    key_ref[...] = bs
    decay_ref[...] = decay
    for store in stores:
        store.start()
    row = lax.broadcasted_iota(jnp.int32, (seqs, width), 0)
    readout = [jnp.zeros((seqs, width), f32) for _ in range(groups)]
    for s in range(seqs):
        if s % batch == 0:
            state_loads[s // batch].wait()
        for g in range(groups):
            block = state[s, g * per_group : (g + 1) * per_group].reshape(width, state_dim)
            read = dot_nt(queries[:, g * state_dim : (g + 1) * state_dim], block.astype(bf16))
            readout[g] = jnp.where(row == s, read, readout[g])
    load_z.wait()
    z_gate = silu(projected(w_z))
    skip = spread_heads(d_skip_ref[...], head_dim) * xs
    kept = spread_heads(decay, head_dim)
    mixed = []
    for g in range(groups):
        part = slice(g * width, (g + 1) * width)
        own = slice(g * state_dim, (g + 1) * state_dim)
        match = jnp.sum(bs[:, own] * cs[:, own], axis=1, keepdims=True)
        read = kept[:, part] * readout[g] + scaled[:, part] * match
        gated = (read + skip[:, part]) * z_gate[:, part]
        mixed.append(rms_rows(gated, group_gain_ref[:, part]).astype(bf16))
    load_out.wait()
    part_ref[...] = dot(jnp.concatenate(mixed, axis=1), w_out[...]).astype(bf16)
    for store in stores:
        store.wait()


def advance_kernel(
    scaled_hbm,
    key_hbm,
    decay_hbm,
    state_hbm,
    state_out,
    scaled_ref,
    key_ref,
    decay_ref,
    state,
    small_sems,
    in_sems,
    out_sems,
):
    seqs, heads, head_dim, state_dim = state.shape
    per_group = heads * state_dim // key_ref.shape[1]
    copy = pltpu.make_async_copy
    small_loads = [
        copy(scaled_hbm, scaled_ref, small_sems.at[0]),
        copy(key_hbm, key_ref, small_sems.at[1]),
        copy(decay_hbm, decay_ref, small_sems.at[2]),
    ]
    batch = max(1, seqs // 4)
    spans = [pl.ds(first, batch) for first in range(0, seqs, batch)]
    loads = [copy(state_hbm.at[p], state.at[p], in_sems.at[i]) for i, p in enumerate(spans)]
    stores = [copy(state.at[p], state_out.at[p], out_sems.at[i]) for i, p in enumerate(spans)]
    for load in [*small_loads, *loads]:
        load.start()
    for load in small_loads:
        load.wait()
    scaled = scaled_ref[...].T
    keys = key_ref[...]
    decay = decay_ref[...]
    for s in range(seqs):
        if s % batch == 0:
            loads[s // batch].wait()
        for h in range(heads):
            g = h // per_group
            key = keys[s : s + 1, g * state_dim : (g + 1) * state_dim]
            column = scaled[h * head_dim : (h + 1) * head_dim, s : s + 1]
            state[s, h] = decay[s : s + 1, h : h + 1] * state[s, h] + column * key
        if (s + 1) % batch == 0:
            stores[s // batch].start()
    for store in stores:
        store.wait()


def norm_kernel(tokens_ref, own_ref, other_ref, gain_ref, packed_ref, spread_ref, residual_ref):
    _, model = tokens_ref.shape
    summed = own_ref[...].astype(f32) + other_ref[...].astype(f32)
    residual = (tokens_ref[...].astype(f32) + summed).astype(bf16)
    residual_ref[...] = residual
    normed = rms_rows(residual.astype(f32), gain_ref[...])
    tiles = jnp.concatenate(
        [normed[:, k * LANES : (k + 1) * LANES] for k in range(model // LANES)], axis=0
    ).astype(bf16)
    count = tiles.shape[0]
    for chip in range(packed_ref.shape[0]):
        spread_ref[chip, :count] = tiles
        spread_ref[chip, count:] = packed_ref[chip]


def token_rows(tiles_ref, seqs, model):
    rows = []
    for chip in range(tiles_ref.shape[0]):
        tiles = tiles_ref[chip, : seqs * model // LANES]
        rows.append(
            jnp.concatenate(
                [tiles[k * seqs : (k + 1) * seqs] for k in range(model // LANES)], axis=1
            )
        )
    return jnp.concatenate(rows, axis=0)


def unfold(packed_ref, parity, start, share, wide_ref):
    chips = packed_ref.shape[0]
    rows = wide_ref.shape[0] // (2 * chips)
    fold = fold_of(rows, share)
    height = rows // fold
    wide_ref[...] = jnp.zeros(wide_ref.shape, bf16)
    for chip in range(chips):
        source = (2 * chip + parity) * rows
        values = packed_ref[chip, start : start + height]
        wide_ref[pl.ds(pl.multiple_of(source, 8), height)] = values
        wider = values.astype(f32)
        for k in range(1, fold):
            moved = pltpu.roll(wider, LANES - k * LANES // fold, 1).astype(bf16)
            wide_ref[pl.ds(pl.multiple_of(source + k * height, 8), height)] = moved


def down_rows(own_ref, other_ref, first, start, share, rows):
    fold = back_fold_of(rows, share)
    height, stride = share // fold, LANES // fold
    pieces = []
    for chip in range(own_ref.shape[0]):
        own, other = [
            jnp.concatenate(
                [values[:, k * stride : k * stride + rows] for k in range(fold)], axis=0
            )
            for values in (
                own_ref[chip, start : start + height].astype(f32),
                other_ref[chip, start : start + height].astype(f32),
            )
        ]
        pieces += [jnp.where(first, own, other), jnp.where(first, other, own)]
    return jnp.concatenate(pieces, axis=1).astype(bf16)


def experts_kernel(core_ref, got_ref, branch_ref, *refs, share, seqs, model):
    gate, up, other_gate, other_up, other_down = refs[:5]
    result_ref, rows_ref, hidden_ref, scale_ref, active_ref, weight_ref, wide_ref = refs[5:]
    chips, total, _ = got_ref.shape
    core = core_ref[0]
    rows = token_rows(got_ref, seqs, model)
    rows_ref[...] = rows
    table = jnp.concatenate(
        [got_ref[i, total - seqs :].astype(f32) for i in range(chips)], axis=0
    )
    lane = lax.broadcasted_iota(jnp.int32, table.shape, 1)

    def active(gate_ref, up_ref):
        return (silu(dot(rows, gate_ref[0])) * dot(rows, up_ref[0])).astype(bf16)

    def weight_of(expert):
        return jnp.sum(jnp.where(lane // 2 == expert, table, 0.0), axis=1, keepdims=True)

    active_ref[...] = active(gate, up)
    weight_ref[...] = jnp.broadcast_to(weight_of(core), weight_ref.shape)
    result_ref[...] = weight_of(1 - core) * dot(active(other_gate, other_up), other_down[0])
    branch = sigmoid(
        jnp.sum(rows.astype(f32) * branch_ref[...].astype(f32)[None], axis=1, keepdims=True)
    )
    scale_ref[...] = jnp.broadcast_to(branch, scale_ref.shape)
    unfold(got_ref, core, seqs * model // LANES, share, wide_ref)
    hidden_ref[...] = dot(rows, wide_ref[...])


def dense_kernel(
    core_ref,
    own_ref,
    other_ref,
    routed_ref,
    rows_ref,
    half_ref,
    scale_ref,
    active_ref,
    weight_ref,
    down_ref,
    out_ref,
    wide_ref,
    *,
    share,
    seqs,
    n_tp,
):
    model = wide_ref.shape[0]
    chips = other_ref.shape[0]
    rows = model // (2 * chips)
    core = core_ref[0]
    start = seqs * model // LANES
    unfold(other_ref, 1 - core, start, share, wide_ref)
    hidden = half_ref[...] + dot(rows_ref[...], wide_ref[...])
    dense = silu(hidden) * pltpu.roll(hidden, LANES - share, 1)
    start += rows // fold_of(rows, share)
    back = down_rows(own_ref, other_ref, core == 0, start, share, rows)
    dense_out = dot(dense[:, :share].astype(bf16), back)
    own_out = weight_ref[:, :1] * dot(active_ref[...], down_ref[0])
    result = routed_ref[...] + own_out + scale_ref[:, :1] * dense_out
    half = model // n_tp
    for i in range(chips):
        for q in range(n_tp):
            place = (i * n_tp + q) * seqs
            value = result[i * seqs : (i + 1) * seqs, q * half : (q + 1) * half]
            out_ref[place : place + seqs] = value.astype(bf16)


def sum_kernel(tp_ref, parts_ref, residual_ref, out_ref, *, n_tp):
    seqs, half = out_ref.shape
    own = tp_ref[0]
    total = jnp.zeros((seqs, half), f32)
    for q in range(n_tp):
        total += jnp.where(
            own == q, residual_ref[:, q * half : (q + 1) * half].astype(f32), 0.0
        )
    for i in range(parts_ref.shape[0] // seqs):
        total += parts_ref[i * seqs : (i + 1) * seqs].astype(f32)
    out_ref[...] = total.astype(bf16)


def body(
    tokens,
    ssm_state,
    conv_x,
    conv_b,
    conv_c,
    w_x,
    w_z,
    w_b,
    w_c,
    w_dt,
    dt_bias,
    a_log,
    d_skip,
    taps_x,
    taps_b,
    taps_c,
    norm1_gain,
    group_gain,
    w_out,
    norm2_gain,
    route_ids,
    route_weights,
    exp_gate,
    exp_up,
    exp_down,
    dense_gate,
    dense_up,
    dense_down,
    branch_gate,
):
    seqs, model = tokens.shape
    n_ep = lax.axis_size("ep")
    n_tp = lax.axis_size("tp")
    tp_index = lax.axis_index("tp").astype(jnp.int32)[None]
    core_index = (lax.axis_index("ep") % 2).astype(jnp.int32)[None]
    sds = jax.ShapeDtypeStruct

    rows, hidden = dense_gate.shape
    chips = n_ep // 2
    share = hidden // chips
    block = packed_rows(rows, share, seqs)
    groups = [[2 * chip + core for chip in range(chips)] for core in range(2)]
    swap = [(i, i ^ 1) for i in range(n_ep)]
    held = (
        tokens,
        norm1_gain[None],
        w_dt.T,
        dt_bias[None],
        a_log[None],
        d_skip[None],
        taps_x,
        taps_b,
        taps_c,
        group_gain[None],
        taps_first(conv_x),
        taps_first(conv_b),
        taps_first(conv_c),
        dense_gate,
        dense_up,
        dense_down.T,
        route_ids,
        route_weights,
        w_x,
        w_b,
        w_c,
        w_z,
        w_out,
        ssm_state,
    )
    results = (
        sds((seqs, w_x.shape[1]), f32),
        sds((seqs, w_b.shape[1]), f32),
        sds((seqs, ssm_state.shape[1]), f32),
        *[sds(taps_first(value).shape, bf16) for value in (conv_x, conv_b, conv_c)],
    )
    part, packed, scaled, keys, decay, conv_x_next, conv_b_next, conv_c_next = pl.pallas_call(
        functools.partial(mixer_kernel, n_tp=n_tp, held=len(held)),
        out_shape=(
            sds((seqs, model), bf16),
            sds((chips, block, LANES), bf16),
            *[pltpu.HBM(value.shape, value.dtype) for value in results],
        ),
        in_specs=[SMEM] + [HBM] * len(held),
        out_specs=(VMEM,) * 2 + (HBM,) * 6,
        scratch_shapes=[pltpu.VMEM(value.shape, value.dtype) for value in held]
        + [pltpu.VMEM(value.shape, value.dtype) for value in results]
        + [
            pltpu.SemaphoreType.DMA((len(held) - 1,)),
            pltpu.SemaphoreType.DMA((seqs,)),
            pltpu.SemaphoreType.DMA((len(results),)),
        ],
        compiler_params=pltpu.CompilerParams(vmem_limit_bytes=20 * MIB),
        name="mixer",
    )(tp_index, *map(in_hbm, held))

    state_next = pl.pallas_call(
        advance_kernel,
        out_shape=sds(ssm_state.shape, f32),
        in_specs=[HBM] * 4,
        out_specs=HBM,
        scratch_shapes=[
            *[pltpu.VMEM(value.shape, f32) for value in (scaled, keys, decay, ssm_state)],
            pltpu.SemaphoreType.DMA((3,)),
            pltpu.SemaphoreType.DMA((seqs,)),
            pltpu.SemaphoreType.DMA((seqs,)),
        ],
        compiler_params=pltpu.CompilerParams(vmem_limit_bytes=12 * MIB),
        name="advance",
    )(*map(in_hbm, (scaled, keys, decay, ssm_state)))

    if n_tp == 2:
        other = lax.ppermute(part, "tp", [(0, 1), (1, 0)])
    else:
        gathered = lax.all_gather(part, "tp", axis=0).astype(f32)
        total = gathered[0]
        for i in range(1, n_tp):
            total = total + gathered[i]
        other = total - part.astype(f32)

    tile_rows = seqs * model // LANES
    spread, residual = pl.pallas_call(
        norm_kernel,
        out_shape=(sds((chips, tile_rows + block, LANES), bf16), sds((seqs, model), bf16)),
        in_specs=[VMEM] * 5,
        out_specs=(VMEM, VMEM),
        compiler_params=pltpu.CompilerParams(vmem_limit_bytes=4 * MIB),
        name="norm",
    )(tokens, part, other, norm2_gain[None], packed)
    got = lax.all_to_all(
        spread, "ep", split_axis=0, concat_axis=0, tiled=True, axis_index_groups=groups
    )
    own_experts = (exp_gate, exp_up, exp_down)
    other_experts = [lax.ppermute(value, "ep", swap) for value in own_experts]
    got_other = lax.ppermute(got, "ep", swap)

    dense_inputs = pl.pallas_call(
        functools.partial(experts_kernel, share=share, seqs=seqs, model=model),
        out_shape=(
            sds((chips * seqs, model), f32),
            sds((chips * seqs, model), bf16),
            sds((chips * seqs, LANES), f32),
            sds((chips * seqs, LANES), f32),
            sds((chips * seqs, exp_gate.shape[2]), bf16),
            sds((chips * seqs, LANES), f32),
        ),
        in_specs=[SMEM] + [VMEM] * 7,
        out_specs=(VMEM,) * 6,
        scratch_shapes=[
            pltpu.VMEM((model, LANES), bf16),
        ],
        compiler_params=pltpu.CompilerParams(vmem_limit_bytes=12 * MIB),
        cost_estimate=pl.CostEstimate(flops=10**10, bytes_accessed=10**6, transcendentals=0),
        name="experts",
    )(core_index, got, branch_gate, exp_gate, exp_up, *other_experts)
    outgoing = pl.pallas_call(
        functools.partial(dense_kernel, share=share, seqs=seqs, n_tp=n_tp),
        out_shape=sds((chips * n_tp * seqs, model // n_tp), bf16),
        in_specs=[SMEM] + [VMEM] * 9,
        out_specs=VMEM,
        scratch_shapes=[pltpu.VMEM((model, LANES), bf16)],
        compiler_params=pltpu.CompilerParams(vmem_limit_bytes=8 * MIB),
        name="dense",
    )(core_index, got, got_other, *dense_inputs, exp_down)
    flat_groups = [[ep * n_tp + q for ep in group for q in range(n_tp)] for group in groups]
    parts = lax.all_to_all(
        outgoing,
        ("ep", "tp"),
        split_axis=0,
        concat_axis=0,
        tiled=True,
        axis_index_groups=flat_groups,
    )

    mixed = pl.pallas_call(
        functools.partial(sum_kernel, n_tp=n_tp),
        out_shape=sds((seqs, model // n_tp), bf16),
        in_specs=[SMEM, VMEM, VMEM],
        out_specs=VMEM,
        compiler_params=pltpu.CompilerParams(vmem_limit_bytes=4 * MIB),
        name="total",
    )(tp_index, parts, residual)
    return (
        mixed,
        state_next,
        taps_first(conv_x_next),
        taps_first(conv_b_next),
        taps_first(conv_c_next),
    )


def solution(mesh):
    return jax.shard_map(
        body,
        mesh=mesh,
        in_specs=(
            P("ep", None),
            P("ep", "tp", None, None),
            P("ep", None, "tp"),
            P("ep", None, "tp"),
            P("ep", None, "tp"),
            P(None, "tp"),
            P(None, "tp"),
            P(None, "tp"),
            P(None, "tp"),
            P(),
            P("tp"),
            P("tp"),
            P("tp"),
            P(None, "tp"),
            P(None, "tp"),
            P(None, "tp"),
            P(),
            P("tp"),
            P("tp", None),
            P(),
            P("ep", None),
            P("ep", None),
            P("ep", None, "tp"),
            P("ep", None, "tp"),
            P("ep", "tp", None),
            P("ep", "tp"),
            P("ep", "tp"),
            P("tp", "ep"),
            P(),
        ),
        out_specs=(
            P("ep", "tp"),
            P("ep", "tp", None, None),
            P("ep", None, "tp"),
            P("ep", None, "tp"),
            P("ep", None, "tp"),
        ),
        check_vma=False,
    )
```
